32 devices in a mesh: ep: 8 (over z, core), tp: 4 (over y, x).
Axes of the slice: x: 2, y: 2, z: 4, core: 2. Of those that a mesh axis runs over, the one named last changes fastest.
Arguments:
- mix_input: bfloat16 [1024, 2048], P('ep'), may hold values from -8 to 8
- expert_input: bfloat16 [1024, 2048], P('ep'), may hold values from -8 to 8
- mix_gain: float32 [2048], replicated, may hold values from 0.1 to 1.9
- moe_gain: float32 [2048], replicated, may hold values from 0.1 to 1.9
- pool_in: bfloat16 [2048, 1024], P(None, 'tp'), may hold values from -0.125 to 0.125
- pool_scale: float32 [1024], P('tp'), may hold values from 0.25 to 10
- pool_gain: float32 [1024], P('tp'), may hold values from 0.1 to 1.9
- pool_out: bfloat16 [1024, 2048], P(None, 'tp'), may hold values from -0.1875 to 0.1875
- route: int32 [1024, 4], P('ep'), may hold values from 0 to 7, all different within a row; in each aligned block of 128 rows (0 to 127, 128 to 255, ...) at most 128 rows name the same one
- route_score: float32 [1024, 4], P('ep'), may hold values from 0.05 to 1
- expert_gate: bfloat16 [8, 2048, 2048], P('ep', None, 'tp'), may hold values from -0.125 to 0.125
- expert_up: bfloat16 [8, 2048, 2048], P('ep', None, 'tp'), may hold values from -0.125 to 0.125
- expert_down: bfloat16 [8, 2048, 2048], P('ep', 'tp'), may hold values from -0.1875 to 0.1875
- shared_gate: bfloat16 [2048, 2048], P(None, 'tp'), may hold values from -0.125 to 0.125
- shared_up: bfloat16 [2048, 2048], P(None, 'tp'), may hold values from -0.125 to 0.125
- shared_down: bfloat16 [2048, 2048], P(None, 'tp'), may hold values from -0.125 to 0.125
Outputs:
- mix_out: bfloat16 [1024, 2048], P('ep', 'tp')
- moe_out: bfloat16 [1024, 2048], P('ep', 'tp')
The draws below stay inside these ranges and needn't reach their ends.
Inputs may be any that keep to these rules, and one draw needn't show every extreme that they name: `route`: each row names 4 different experts. In the rows of one index of ep (aligned blocks of 128 rows) no expert is named more than 128 times, a bound that some block reaches.
All inputs are finite; a program needn't handle non-finite values.
Results may differ from the reference program's by a relative error of at most 0.014.
Values may be sent and summed in bfloat16 or wider, within the bound.
A program may use at most 64 MiB of HBM per device.

```python
import math
import jax
import jax.numpy as jnp
import numpy as np
from jax import lax

D = 2048
POOL = 1024
FE = 2048
FS = 2048
TOP_K = 4
TOK_B = 128
EXPERTS = 8
CAP = 128
TOKENS_A = 1024
TOKENS_B = 1024
N_EP = 8
N_TP = 4


def spread_rows(key, rows, cols):
    keys = jax.random.split(key, 3)
    row_scale = jnp.exp(jax.random.uniform(keys[0], (rows, 1), jnp.float32, math.log(0.3), math.log(3.0)))
    col_scale = jnp.exp(jax.random.uniform(keys[1], (1, cols), jnp.float32, math.log(0.3), math.log(3.0)))
    base = jax.random.normal(keys[2], (rows, cols), jnp.float32)
    return jnp.clip(base * row_scale * col_scale, -8.0, 8.0).astype(jnp.bfloat16)


def draw_mix_input(key, part):
    return spread_rows(jax.random.fold_in(key, 11), TOKENS_A, D)


def draw_expert_input(key, part):
    return spread_rows(jax.random.fold_in(key, 23), TOKENS_B, D)


def draw_pool_scale(key, part):
    channel = jnp.arange(POOL, dtype=jnp.float32) / POOL
    factor = jnp.exp(jax.random.uniform(jax.random.fold_in(key, 37), (POOL,), jnp.float32, math.log(0.5), math.log(2.0)))
    rising = jnp.exp(math.log(6.0) * channel)
    return 0.5 * rising * factor


def with_spikes(values, own_key, source, target, blocks, factor):
    def block_of(axis_at):
        return (jnp.arange(values.shape[axis_at]) // (values.shape[axis_at] // blocks)).reshape((-1,) + (1,) * (values.ndim - 1 - axis_at))

    near = jax.random.permutation(own_key, blocks)[block_of(target)]
    other_side = (block_of(target) + blocks // 2) % blocks
    return jnp.where((block_of(source) == near) | (block_of(source) == other_side), factor * values, values)


def steps_of(own_key, extent, cuts, low, top_value):
    loudness, own = 1.0, jax.random.fold_in(own_key, 6)
    for axis_at, blocks in cuts:
        steps = jnp.exp(jax.random.uniform(jax.random.fold_in(own, axis_at), (blocks,), jnp.float32, low / len(cuts), top_value / len(cuts)))
        loudness = loudness * jnp.repeat(steps, extent[axis_at] // blocks).reshape([-1 if axis == axis_at else 1 for axis in range(len(extent))])
    return loudness


def routed_block(own_key, own, number, rows, number_of, top, reach, slope):
    order = jax.random.permutation(own_key, number_of)
    heavy_load, usual = load_shares(number_of, rows * top, reach, slope, True), load_shares(number_of, rows * top, reach, slope, False)
    places = jnp.arange(number_of)

    def named(tallies, turn):
        used = int((tallies > 0).sum())
        fixed = max(1, used // 4)
        passed = fixed + (places - fixed + turn * (used - fixed)) % max(1, number_of - fixed)
        return jnp.zeros((number_of,), jnp.int32).at[order[jnp.where(places < fixed, places, passed)]].set(jnp.asarray(tallies, jnp.int32))

    tallies = jnp.where(number % 4 == 0, named(heavy_load, number // 4), named(usual, number - number // 4 - 1))
    mixed = jax.random.permutation(jax.random.fold_in(own, 3), number_of)
    source_of, receiver = mixed[0:number_of // 2 * 2:2], mixed[1:number_of // 2 * 2:2]
    slack = jnp.minimum(tallies[source_of] - 1, reach - tallies[receiver]) // 2
    slack = jnp.where((source_of == order[0]) | (receiver == order[0]) | (tallies[receiver] == 0), 0, jnp.maximum(slack, 0))
    passed = jax.random.randint(jax.random.fold_in(own, 4), (number_of // 2,), 0, 1 << 20) % (slack + 1)
    tallies = tallies.at[source_of].add(-passed).at[receiver].add(passed)
    items = jnp.searchsorted(jnp.cumsum(tallies), jnp.arange(rows * top), side="right").astype(jnp.int32)
    grid = items.reshape(top, rows).T
    grid = grid[jax.random.permutation(jax.random.fold_in(own, 1), rows)]
    turn = jax.random.randint(jax.random.fold_in(own, 2), (rows, 1), 0, top)
    return jnp.take_along_axis(grid, (jnp.arange(top)[None, :] + turn) % top, axis=1)


def load_shares(number_of, total, most, skew, full):
    loads = [(1 << 20) // math.isqrt(grade ** skew) + 1 for grade in range(1, number_of + 1)]
    largest = most if full else min(most, max(-(-total // number_of), total * loads[0] // sum(loads)))
    least = 1 if total - largest >= number_of - 1 else 0
    given, rest = [largest] + [least] * (number_of - 1), total - largest - least * (number_of - 1)
    while rest > 0:
        candidates = [i for i in range(1, number_of) if given[i] < largest] or [i for i in range(1, number_of) if given[i] < most]
        mass, budget = sum([loads[i] for i in candidates]), rest
        for i in candidates:
            more = min(most - given[i], max(1, budget * loads[i] // mass), rest)
            given[i] = given[i] + more
            rest = rest - more
    return np.array(given)


def bell_draw(stream_key, shape, spread, bound, pieces=(), kind=jnp.bfloat16):
    values = spread * jax.random.normal(stream_key, shape, jnp.float32)
    if pieces:
        values = values * steps_of(stream_key, shape, pieces, -0.22, 0.18)
    return jnp.clip(values, -bound, bound).astype(kind)


def gaussian_with(own_key, dims, deviation, reach, pieces, heavy, held_as=jnp.bfloat16):
    values = deviation * jax.random.normal(own_key, dims, jnp.float32)
    if pieces:
        values = values * steps_of(own_key, dims, pieces, -0.22, 0.18)
    return jnp.clip(with_spikes(values, jax.random.fold_in(own_key, 3), *heavy), -reach, reach).astype(held_as)


def setup_inputs(seed: int = 0) -> dict:
    arg_keys = jax.random.split(jax.random.key(seed), 17)
    mix_input = draw_mix_input(jax.random.fold_in(arg_keys[16], 71), 0)
    expert_input = draw_expert_input(jax.random.fold_in(arg_keys[16], 71), 0)
    mix_gain = jnp.clip(1.0 + 0.18 * jax.random.normal(arg_keys[2], (D,), jnp.float32), 0.1, 1.9)
    moe_gain = jnp.clip(1.0 + 0.18 * jax.random.normal(arg_keys[3], (D,), jnp.float32), 0.1, 1.9)
    pool_in = bell_draw(arg_keys[4], (D, POOL), D ** -0.5, 0.125, ((1, 4),))
    pool_scale = draw_pool_scale(jax.random.fold_in(arg_keys[16], 71), 0)
    pool_gain = jnp.clip(1.0 + 0.18 * jax.random.normal(arg_keys[6], (POOL,), jnp.float32), 0.1, 1.9)
    pool_out = bell_draw(arg_keys[7], (POOL, D), POOL ** -0.5, 0.1875, ((1, 4),))
    route_keys = jax.random.split(jax.random.fold_in(arg_keys[8], 1), TOKENS_B // TOK_B)
    route_turns = jax.random.permutation(jax.random.fold_in(arg_keys[8], 3), TOKENS_B // TOK_B)
    route = jax.vmap(lambda own, number: routed_block(jax.random.fold_in(arg_keys[8], 2), own, number, TOK_B, EXPERTS, TOP_K, CAP, 2))(route_keys, route_turns).reshape((TOKENS_B, TOP_K))
    route_score = jnp.clip(0.05 + 0.95 * jax.random.uniform(arg_keys[9], (TOKENS_B, TOP_K), jnp.float32) ** steps_of(arg_keys[9], (TOKENS_B, TOP_K), ((0, 8),), -0.2, 0.2), 0.05, 1.0)
    expert_gate = bell_draw(arg_keys[10], (EXPERTS, D, FE), D ** -0.5, 0.125, ((0, 8), (2, 4)))
    expert_up = bell_draw(arg_keys[11], (EXPERTS, D, FE), D ** -0.5, 0.125, ((0, 8), (2, 4)))
    expert_down = gaussian_with(arg_keys[12], (EXPERTS, FE, D), FE ** -0.5, 0.1875, ((0, 8), (1, 4)), (1, 2, 4, 2.0))
    shared_gate = bell_draw(arg_keys[13], (D, FS), D ** -0.5, 0.125, ((1, 4),))
    shared_up = bell_draw(arg_keys[14], (D, FS), D ** -0.5, 0.125, ((1, 4),))
    shared_down = bell_draw(arg_keys[15], (FS, D), FS ** -0.5, 0.125, ((1, 4),))
    return {"mix_input": mix_input, "expert_input": expert_input, "mix_gain": mix_gain, "moe_gain": moe_gain, "pool_in": pool_in, "pool_scale": pool_scale, "pool_gain": pool_gain, "pool_out": pool_out, "route": route, "route_score": route_score, "expert_gate": expert_gate, "expert_up": expert_up, "expert_down": expert_down, "shared_gate": shared_gate, "shared_up": shared_up, "shared_down": shared_down}


epsilon = 1e-06
reach_rows = 15
window_widths = (2, 4, 8, 16)

def row_norm(rows, gain):
    values = rows.astype(jnp.float32)
    scale = lax.rsqrt(lax.optimization_barrier(jnp.mean(values * values, axis=-1, keepdims=True)) + epsilon)
    return (values * scale * gain.astype(jnp.float32)).astype(jnp.bfloat16)

def window_means(extended, position, group, n_rows):
    total = jnp.zeros((n_rows, extended.shape[1]), jnp.float32)
    result = jnp.zeros((n_rows, extended.shape[1]), jnp.float32)
    for lag in range(16):
        total = total + extended[reach_rows - lag:reach_rows - lag + n_rows]
        for index, width in enumerate(window_widths):
            if lag + 1 == width:
                count = jnp.minimum(position, float(width))[:, None]
                result = jnp.where(group[None, :] == index, total / count, result)
    return result - extended[reach_rows:]

def reference(mix_input, expert_input, mix_gain, moe_gain, pool_in, pool_scale, pool_gain, pool_out, route, route_score, expert_gate, expert_up, expert_down, shared_gate, shared_up, shared_down):
    mix_norm = row_norm(mix_input, mix_gain)
    pool_input = jnp.dot(mix_norm, pool_in, preferred_element_type=jnp.float32).astype(jnp.bfloat16)
    extended = jnp.concatenate([jnp.zeros((reach_rows, POOL), jnp.float32), pool_input.astype(jnp.float32)], axis=0)
    position = jnp.arange(1, TOKENS_A + 1, dtype=jnp.int32).astype(jnp.float32)
    group = jnp.arange(POOL, dtype=jnp.int32) // (POOL // 4)
    scaled = window_means(extended, position, group, TOKENS_A) * pool_scale
    pooled_norm = (scaled * lax.rsqrt(lax.optimization_barrier(jnp.mean(scaled * scaled, axis=1, keepdims=True)) + epsilon) * pool_gain).astype(jnp.bfloat16)
    mix_out = jnp.dot(pooled_norm, pool_out, preferred_element_type=jnp.float32).astype(jnp.bfloat16)
    moe_norm = row_norm(expert_input, moe_gain)
    weights = 2.5 * route_score / lax.optimization_barrier(jnp.sum(route_score, axis=1, keepdims=True))
    most_rows = CAP * N_EP

    def one_expert(routed, expert):
        hit = route == expert
        taken = jnp.any(hit, axis=1)
        order = jnp.argsort(jnp.where(taken, 0, 1).astype(jnp.int32), stable=True)[:most_rows].astype(jnp.int32)
        live = taken[order]
        rows = moe_norm[order]
        gate = jnp.dot(rows, expert_gate[expert], preferred_element_type=jnp.float32)
        upper = jnp.dot(rows, expert_up[expert], preferred_element_type=jnp.float32)
        hidden = (jax.nn.silu(gate) * upper).astype(jnp.bfloat16)
        blocks = hidden.reshape(most_rows, N_TP, FE // N_TP).astype(jnp.float32)
        down = expert_down[expert].reshape(N_TP, FE // N_TP, D).astype(jnp.float32)
        partial_value = jnp.einsum('rpf,pfd->rpd', blocks, down).astype(jnp.bfloat16)
        result = lax.optimization_barrier(jnp.sum(partial_value.astype(jnp.float32), axis=1)).astype(jnp.bfloat16)
        factor = lax.optimization_barrier(jnp.sum(jnp.where(hit, weights, 0.0), axis=1))[order] * live
        routed = routed.at[order].add(result.astype(jnp.float32) * factor[:, None])
        return (routed, None)
    routed, _ = lax.scan(one_expert, jnp.zeros((TOKENS_B, D), jnp.float32), jnp.arange(EXPERTS, dtype=jnp.int32))
    shared_hidden = (jax.nn.silu(jnp.dot(moe_norm, shared_gate, preferred_element_type=jnp.float32)) * jnp.dot(moe_norm, shared_up, preferred_element_type=jnp.float32)).astype(jnp.bfloat16)
    shared = jnp.dot(shared_hidden, shared_down, preferred_element_type=jnp.float32)
    moe_out = (routed + shared).astype(jnp.bfloat16)
    return (mix_out, moe_out)
```

```python
import jax
import jax.numpy as jnp
from jax import lax
from jax.experimental import pallas as pl
from jax.experimental.pallas import tpu as pltpu
from jax.sharding import PartitionSpec as P

epsilon = 1e-06
reach_rows = 15
window_widths = (2, 4, 8, 16)


def shifted(block, axis, distance):
    devices = range(lax.axis_size(axis))
    route = [(i - distance, i) for i in devices if i - distance in devices]
    return lax.ppermute(block, axis, route)


def row_norm(rows, gain):
    values = rows.astype(jnp.float32)
    scale = lax.rsqrt(jnp.mean(values * values, axis=-1, keepdims=True) + epsilon)
    return (values * scale * gain).astype(jnp.bfloat16)


def window_means(extended, position, group, n_rows):
    total = jnp.zeros((n_rows, extended.shape[1]), jnp.float32)
    result = jnp.zeros((n_rows, extended.shape[1]), jnp.float32)
    for lag in range(16):
        total = total + extended[reach_rows - lag : reach_rows - lag + n_rows]
        for index, width in enumerate(window_widths):
            if lag + 1 == width:
                count = jnp.minimum(position, float(width))[:, None]
                result = jnp.where(group[None, :] == index, total / count, result)
    return result - extended[reach_rows:]


def serve(sending, expert_gate, expert_up, expert_down):
    arrived = lax.all_to_all(sending, "ep", split_axis=0, concat_axis=0, tiled=True)
    gate = jnp.einsum("send,edf->senf", arrived, expert_gate, preferred_element_type=jnp.float32)
    upper = jnp.einsum("send,edf->senf", arrived, expert_up, preferred_element_type=jnp.float32)
    hidden = (jax.nn.silu(gate) * upper).astype(jnp.bfloat16)
    term = jnp.einsum("senf,efd->send", hidden, expert_down, preferred_element_type=jnp.float32)
    summed = lax.psum_scatter(term.astype(jnp.bfloat16), "tp", scatter_dimension=3, tiled=True)
    return lax.all_to_all(summed, "ep", split_axis=0, concat_axis=0, tiled=True)


def on_device(
    mix_input,
    expert_input,
    mix_gain,
    moe_gain,
    pool_in,
    pool_scale,
    pool_gain,
    pool_out,
    route,
    route_score,
    expert_gate,
    expert_up,
    expert_down,
    shared_gate,
    shared_up,
    shared_down,
):
    tok_rows = mix_input.shape[0]
    channels = pool_in.shape[1]
    pool_width = channels * lax.axis_size("tp")
    mix_norm = row_norm(mix_input, mix_gain)
    pool_input = jnp.dot(mix_norm, pool_in, preferred_element_type=jnp.float32).astype(jnp.bfloat16)
    before = shifted(pool_input[tok_rows - reach_rows :], "ep", 1)
    extended = jnp.concatenate([before, pool_input], axis=0).astype(jnp.float32)
    position = (lax.axis_index("ep") * tok_rows + jnp.arange(tok_rows, dtype=jnp.int32) + 1).astype(
        jnp.float32
    )
    channel_ids = lax.axis_index("tp") * channels + jnp.arange(channels, dtype=jnp.int32)
    group = channel_ids // (pool_width // 4)
    scaled = window_means(extended, position, group, tok_rows) * pool_scale
    squares = lax.psum(jnp.sum(scaled * scaled, axis=1), "tp")
    pooled_norm = (scaled * lax.rsqrt(squares / pool_width + epsilon)[:, None] * pool_gain).astype(
        jnp.bfloat16
    )
    moe_norm = row_norm(expert_input, moe_gain)
    shared_hidden = (
        jax.nn.silu(jnp.dot(moe_norm, shared_gate, preferred_element_type=jnp.float32))
        * jnp.dot(moe_norm, shared_up, preferred_element_type=jnp.float32)
    ).astype(jnp.bfloat16)
    pooled_all, shared_all = (
        lax.all_gather(pooled_norm, "tp", axis=1, tiled=True),
        lax.all_gather(shared_hidden, "tp", axis=1, tiled=True),
    )
    mix_out = jnp.dot(pooled_all, pool_out, preferred_element_type=jnp.float32).astype(jnp.bfloat16)
    shared_part = jnp.dot(shared_all, shared_down, preferred_element_type=jnp.float32)
    n_tok, top = route.shape
    local_experts = expert_gate.shape[0]
    experts = local_experts * lax.axis_size("ep")
    capacity = 2 * n_tok * top // experts
    flat_route = route.reshape(-1)
    table = (flat_route[:, None] == jnp.arange(experts, dtype=jnp.int32)[None, :]).astype(jnp.int32)
    ranks = jnp.sum((jnp.cumsum(table, axis=0) - table) * table, axis=1)
    slot = flat_route * capacity + ranks
    owner = (
        jnp.full((experts * capacity,), n_tok, jnp.int32)
        .at[slot]
        .set(jnp.arange(n_tok * top, dtype=jnp.int32) // top)
    )
    padded_rows = jnp.concatenate(
        [moe_norm, jnp.zeros((1, moe_norm.shape[1]), jnp.bfloat16)], axis=0
    )
    outgoing = padded_rows[owner].reshape(
        lax.axis_size("ep"), local_experts, capacity, moe_norm.shape[1]
    )
    middle = capacity // 2
    first = serve(outgoing[:, :, :middle], expert_gate, expert_up, expert_down)
    second = serve(outgoing[:, :, middle:], expert_gate, expert_up, expert_down)
    returned = jnp.concatenate([first, second], axis=2)
    back_rows = returned.reshape(experts * capacity, returned.shape[3])
    picked = back_rows[slot].reshape(n_tok, top, returned.shape[3]).astype(jnp.float32)
    weights = 2.5 * route_score / jnp.sum(route_score, axis=1, keepdims=True)
    routed = jnp.sum(picked * weights[:, :, None], axis=1)
    moe_out = (routed + shared_part).astype(jnp.bfloat16)
    return (mix_out, moe_out)


MESH = pl.DeviceIdType.MESH


def places():
    ep, tp = lax.axis_index("ep"), lax.axis_index("tp")
    z, core = ep // 2, ep % 2
    y, x = tp // 2, tp % 2
    return ep, tp, z, core, y * 2 + 1 - x, (1 - y) * 2 + x, (1 - y) * 2 + 1 - x


def greet(partners):
    barrier = pltpu.get_barrier_semaphore()
    for partner in partners:
        pl.semaphore_signal(barrier, inc=1, device_id=partner, device_id_type=MESH)
    pl.semaphore_wait(barrier, len(partners))


def aligned(start, size):
    return pl.ds(pl.multiple_of(start * size, size), size)


def fused_kernel(n_ep, n_tp, *refs):
    hbm, (mix_ref, moe_ref), rest = refs[:16], refs[16:18], refs[18:]
    (mi_h, ei_h, mg_h, eg_h, pi_h, ps_h, pg_h, po_h, rt_h, sc_h, wg_h, wu_h, wd_h, sg_h, su_h, sd_h) = hbm
    staged, rest = rest[:16], rest[16:]
    (mi, ei, mg, eg, pin, pscale, pgain, pout, rt, sc, wg, wu, wd, sg, su, sd) = staged
    (g, dense, mm, halo_s, halo_r, ext, sh_all, po_all, sq_all, hid) = rest[:10]
    (p, ca, s, bx, by, qx, qy, r, bz, o) = rest[10:20]
    l_sem = rest[20]
    (w_s, w_r, z_s, z_r, gx_s, gx_r, gy_s, gy_r, gu_s, gu_r, gv_s, gv_r, gc_s, gc_r) = rest[21:35]
    (c_s, c_r, dx_s, dx_r, dy_s, dy_r, x_s, x_r, y_s, y_r, f_s, f_r, t_s, t_r, q_s, q_r, h_s, h_r) = rest[35:]
    ep, tp, z, core, xn, yn, dg = places()
    n_z = n_ep // 2
    rows, width = ei.shape
    cols = width // n_tp
    half = rows // 2
    f32, bf16 = jnp.float32, jnp.bfloat16
    other_core = z * 2 + 1 - core
    own_rows = aligned(ep, rows)
    low, high = pl.ds(0, half), pl.ds(half, half)

    loads = {}
    for number in (8, 9, 1, 3, 0, 2, 4, 13, 14, 5, 6, 10, 11, 12, 15, 7):
        loads[number] = pltpu.make_async_copy(hbm[number], staged[number], l_sem.at[number])
        loads[number].start()

    def send(src, dst, sem_s, sem_r, device):
        copy = pltpu.make_async_remote_copy(
            src_ref=src, dst_ref=dst, send_sem=sem_s, recv_sem=sem_r, device_id=device, device_id_type=MESH
        )
        copy.start()
        return copy

    peers = (xn, yn, dg)
    partners = [((ep + m) % n_ep, tp) for m in range(1, n_ep)] + [(ep, t) for t in peers]
    barrier = pltpu.get_barrier_semaphore()
    for partner in partners:
        pl.semaphore_signal(barrier, inc=1, device_id=partner, device_id_type=MESH)

    def norm_into(src, gain, dst, start):
        step = 16

        def some(index, carry):
            values = src[aligned(index, step), :].astype(f32)
            scale = lax.rsqrt(jnp.mean(values * values, axis=-1, keepdims=True) + epsilon)
            dst[pl.ds(pl.multiple_of(start + index * step, step), step), :] = (
                values * scale * gain[...]
            ).astype(bf16)
            return carry

        lax.fori_loop(0, rows // step, some, 0)

    with jax.named_scope("norm"):
        loads[8].wait()
        loads[9].wait()
        total_score = jnp.sum(sc[...], axis=0, keepdims=True)
        expert_ids = lax.broadcasted_iota(jnp.int32, (n_ep, rows), 0)
        mine = jnp.zeros((n_ep, rows), f32)
        for choice in range(rt.shape[0]):
            share = 2.5 * sc[choice : choice + 1, :] / total_score
            mine = mine + jnp.where(rt[choice : choice + 1, :] == expert_ids, share, 0.0)
        dense[ep] = mine
        loads[1].wait()
        loads[3].wait()
        norm_into(ei, eg, g, ep * rows)
    with jax.named_scope("greet"):
        pl.semaphore_wait(barrier, len(partners))
    w_copies = [
        send(dense.at[ep], dense.at[ep], w_s.at[m], w_r.at[m], ((ep + m) % n_ep, tp))
        for m in range(1, n_ep)
    ]
    order = [1, n_z - 1] + list(range(2, n_z - 1))
    z_copies, gx, gy, gu, gv, gc = {}, {}, {}, {}, {}, {}
    for k in order:
        piece = g.at[own_rows, aligned(tp, cols)]
        z_copies[k] = send(piece, piece, z_s.at[k], z_r.at[k], (((z + k) % n_z) * 2 + core, tp))
    whole = g.at[own_rows, :]
    gc[0] = send(whole, whole, gc_s.at[0], gc_r.at[0], (other_core, tp))

    with jax.named_scope("shared"):
        loads[13].wait()
        loads[14].wait()
        fs = sg.shape[1]
        tile = 256

        def shared_tile(index, carry):
            part = aligned(index, tile)
            gate = jnp.dot(g[own_rows, :], sg[:, part], preferred_element_type=f32)
            upper = jnp.dot(g[own_rows, :], su[:, part], preferred_element_type=f32)
            sh_all[:, pl.ds(pl.multiple_of(tp * fs + index * tile, tile), tile)] = (
                gate / (1.0 + jnp.exp(-gate)) * upper
            ).astype(bf16)
            return carry

        lax.fori_loop(0, fs // tile, shared_tile, 0)
    t_copies = {}

    def spread(kind, buffer):
        size = buffer.shape[1] // n_tp
        mine_slot = buffer.at[:, aligned(tp, size)]
        t_copies[kind, 0] = send(mine_slot, mine_slot, t_s.at[kind, 0], t_r.at[kind, 0], (ep, xn))
        t_copies[kind, 1] = send(mine_slot, mine_slot, t_s.at[kind, 1], t_r.at[kind, 1], (ep, yn))

    def spread_corner(kind, buffer):
        size = buffer.shape[1] // n_tp
        t_copies[kind, 0].wait_recv()
        part = buffer.at[low, aligned(xn, size)]
        t_copies[kind, 2] = send(part, part, t_s.at[kind, 2], t_r.at[kind, 2], (ep, yn))
        t_copies[kind, 1].wait_recv()
        part = buffer.at[high, aligned(yn, size)]
        t_copies[kind, 3] = send(part, part, t_s.at[kind, 3], t_r.at[kind, 3], (ep, xn))

    spread(0, sh_all)

    channels = pin.shape[1]
    reach = halo_s.shape[0]
    with jax.named_scope("pool_in"):
        loads[0].wait()
        loads[2].wait()
        norm_into(mi, mg, mm, 0)
        loads[4].wait()
        pooled_in = jnp.dot(mm[...], pin[...], preferred_element_type=f32).astype(bf16)
        halo_s[...] = pooled_in[rows - reach :]
        ext[reach:, :] = pooled_in.astype(f32)
        halo = send(halo_s, halo_r, h_s, h_r, ((ep + 1) % n_ep, tp))

    eye = lax.broadcasted_iota(jnp.int32, (rows, rows), 0) == lax.broadcasted_iota(
        jnp.int32, (rows, rows), 1
    )

    def window():
        halo.wait_recv()
        ext[:reach, :] = jnp.where(ep == 0, 0.0, halo_r[...].astype(f32))
        position = (ep * rows + 1 + lax.broadcasted_iota(jnp.int32, (rows, 1), 0)).astype(f32)
        total = jnp.zeros((rows, channels), f32)
        result = jnp.zeros((rows, channels), f32)
        for lag in range(reach):
            total = total + ext[reach - lag : reach - lag + rows, :]
            for index, size in enumerate(window_widths):
                if lag + 1 == size:
                    count = jnp.minimum(position, float(size))
                    result = jnp.where(tp == index, total / count, result)
        loads[5].wait()
        loads[6].wait()
        scaled = (result - ext[reach:, :]) * pscale[...]
        squares = jnp.sum(scaled * scaled, axis=1, keepdims=True)
        sq_all[tp] = jnp.sum(jnp.where(eye, squares, 0.0), axis=0, keepdims=True)
        po_all[:, aligned(tp, channels)] = (scaled * pgain[...]).astype(bf16)

    def block(k):
        return ((z + n_z - k) % n_z) * 2 + core

    def gathered(k, quarter):
        return g.at[aligned(block(k), rows), aligned(quarter, cols)]

    def gathered_half(k, part, quarter):
        start = pl.multiple_of(block(k) * rows + part * half, half)
        return g.at[pl.ds(start, half), aligned(quarter, cols)]

    def across(k):
        with jax.named_scope(f"across{k}"):
            z_copies[k].wait_recv()
            part = gathered(k, tp)
            gx[k] = send(part, part, gx_s.at[k], gx_r.at[k], (ep, xn))
            gy[k] = send(part, part, gy_s.at[k], gy_r.at[k], (ep, yn))

    def corner(k):
        with jax.named_scope(f"corner{k}"):
            gx[k].wait_recv()
            part = gathered_half(k, 0, xn)
            gu[k] = send(part, part, gu_s.at[k], gu_r.at[k], (ep, yn))
            gy[k].wait_recv()
            part = gathered_half(k, 1, yn)
            gv[k] = send(part, part, gv_s.at[k], gv_r.at[k], (ep, xn))

    def over(k):
        with jax.named_scope(f"over{k}"):
            gu[k].wait_recv()
            gv[k].wait_recv()
            part = g.at[aligned(block(k), rows), :]
            gc[k] = send(part, part, gc_s.at[k], gc_r.at[k], (other_core, tp))

    c_copies, dx_copies, dy_copies, x_copies, y_copies, f_copies = {}, {}, {}, {}, {}, {}
    fe = wg.shape[1]

    def compute(k):
        plane = (z + n_z - k) % n_z
        with jax.named_scope(f"wait_over{k}"):
            gc[k].wait_recv()
        with jax.named_scope(f"hidden{k}"):
            pair = aligned(plane, 2 * rows)
            factors = []
            for part in range(2):
                line = dense[plane * 2 + part, pl.ds(ep, 1), :]
                factors.append(jnp.sum(jnp.where(eye, line, 0.0), axis=1, keepdims=True))
            factor = jnp.concatenate(factors, axis=0)

            def tile_hidden(index, carry):
                part = aligned(index, tile)
                gate = jnp.dot(g[pair, :], wg[:, part], preferred_element_type=f32)
                upper = jnp.dot(g[pair, :], wu[:, part], preferred_element_type=f32)
                hid[:, part] = (gate / (1.0 + jnp.exp(-gate)) * upper * factor).astype(bf16)
                return carry

            lax.fori_loop(0, fe // tile, tile_hidden, 0)
        with jax.named_scope(f"down{k}"):

            def tile_down(index, carry):
                part = aligned(index, cols)
                p[k, :, part] = jnp.dot(hid[...], wd[:, part], preferred_element_type=f32).astype(bf16)
                return carry

            lax.fori_loop(0, width // cols, tile_down, 0)
            c_copies[k] = send(
                p.at[k, aligned(1 - core, rows), :], ca.at[k], c_s.at[k], c_r.at[k], (other_core, tp)
            )

    def first(k):
        with jax.named_scope(f"first{k}"):
            c_copies[k].wait_recv()
            s[k] = (p[k, aligned(core, rows), :].astype(f32) + ca[k].astype(f32)).astype(bf16)
            dx_copies[k] = send(
                s.at[k, low, aligned(dg, cols)], bx.at[k], dx_s.at[k], dx_r.at[k], (ep, xn)
            )
            dy_copies[k] = send(
                s.at[k, high, aligned(dg, cols)], by.at[k], dy_s.at[k], dy_r.at[k], (ep, yn)
            )

    def second(k):
        with jax.named_scope(f"second{k}"):
            dx_copies[k].wait_recv()
            s[k, low, aligned(yn, cols)] = (
                s[k, low, aligned(yn, cols)].astype(f32) + bx[k].astype(f32)
            ).astype(bf16)
            y_copies[k] = send(
                s.at[k, :, aligned(yn, cols)], qy.at[k], y_s.at[k], y_r.at[k], (ep, yn)
            )
            dy_copies[k].wait_recv()
            s[k, high, aligned(xn, cols)] = (
                s[k, high, aligned(xn, cols)].astype(f32) + by[k].astype(f32)
            ).astype(bf16)
            x_copies[k] = send(
                s.at[k, :, aligned(xn, cols)], qx.at[k], x_s.at[k], x_r.at[k], (ep, xn)
            )

    def third(k):
        with jax.named_scope(f"third{k}"):
            x_copies[k].wait_recv()
            y_copies[k].wait_recv()
            total = (
                s[k, :, aligned(tp, cols)].astype(f32) + qx[k].astype(f32) + qy[k].astype(f32)
            )
            if k == 0:
                o[...] += total
            else:
                r[k] = total.astype(bf16)
                f_copies[k] = send(
                    r.at[k], bz.at[k], f_s.at[k], f_r.at[k], (((z + n_z - k) % n_z) * 2 + core, tp)
                )

    q_copies = []

    def finish_t():
        with jax.named_scope("epilogue"):
            for kind in range(2):
                t_copies[kind, 2].wait_recv()
                t_copies[kind, 3].wait_recv()
            for copy in q_copies:
                copy.wait()
            loads[15].wait()
            loads[7].wait()
            o[...] = jnp.dot(sh_all[...], sd[...], preferred_element_type=f32)
            mean = jnp.sum(sq_all[...], axis=0) / (channels * n_tp)
            inverse = lax.rsqrt(mean + epsilon)
            inverse = jnp.sum(jnp.where(eye, inverse, 0.0), axis=1, keepdims=True)
            mix_ref[...] = (
                jnp.dot(po_all[...], pout[...], preferred_element_type=f32) * inverse
            ).astype(bf16)

    with jax.named_scope("w_wait"):
        for copy in w_copies:
            copy.wait()
    with jax.named_scope("weights_wait"):
        for number in (10, 11, 12):
            loads[number].wait()
    with jax.named_scope("window"):
        window()
        spread(1, po_all)
        for number, t in enumerate(peers):
            q_copies.append(send(sq_all.at[tp], sq_all.at[tp], q_s.at[number], q_r.at[number], (ep, t)))

    far = order[2:]
    compute(0)
    across(order[0])
    across(order[1])
    with jax.named_scope("spread_corner"):
        spread_corner(0, sh_all)
        spread_corner(1, po_all)
    first(0)
    for k in far:
        across(k)
    corner(order[0])
    corner(order[1])
    over(order[0])
    over(order[1])
    second(0)
    for k in far:
        corner(k)
    finish_t()
    compute(order[0])
    for k in far:
        over(k)
    first(order[0])
    compute(order[1])
    third(0)
    second(order[0])
    first(order[1])
    todo = order[1:]
    for k in far:
        compute(k)
        second(todo[0])
        first(k)
        third(order[order.index(todo[0]) - 1])
        todo = todo[1:]
    second(order[-1])
    third(order[-2])
    third(order[-1])
    with jax.named_scope("final"):
        for k in order[:-1]:
            f_copies[k].wait_recv()
            o[...] += bz[k].astype(f32)
        f_copies[order[-1]].wait_recv()
        moe_ref[...] = (o[...] + bz[order[-1]].astype(f32)).astype(bf16)
    with jax.named_scope("drain"):
        halo.wait_send()
        for group in (
            z_copies, gx, gy, gu, gv, gc, t_copies,
            c_copies, dx_copies, dy_copies, x_copies, y_copies, f_copies,
        ):
            for copy in group.values():
                copy.wait_send()


def dense_on_device(
    mix_input,
    expert_input,
    mix_gain,
    moe_gain,
    pool_in,
    pool_scale,
    pool_gain,
    pool_out,
    route,
    route_score,
    expert_gate,
    expert_up,
    expert_down,
    shared_gate,
    shared_up,
    shared_down,
):
    n_ep, n_tp = lax.axis_size("ep"), lax.axis_size("tp")
    n_z = n_ep // 2
    operands = (
        mix_input,
        expert_input,
        mix_gain.reshape(1, -1),
        moe_gain.reshape(1, -1),
        pool_in,
        pool_scale.reshape(1, -1),
        pool_gain.reshape(1, -1),
        pool_out,
        route.T,
        route_score.T,
        expert_gate[0],
        expert_up[0],
        expert_down[0],
        shared_gate,
        shared_up,
        shared_down,
    )
    rows, width = expert_input.shape
    cols = width // n_tp
    half = rows // 2
    channels = pool_in.shape[1]
    reach = reach_rows + 1
    f32, bf16 = jnp.float32, jnp.bfloat16
    scratch = [pltpu.VMEM(a.shape, a.dtype) for a in operands] + [
        pltpu.VMEM((n_ep * rows, width), bf16),
        pltpu.VMEM((n_ep, n_ep, rows), f32),
        pltpu.VMEM((rows, width), bf16),
        pltpu.VMEM((reach, channels), bf16),
        pltpu.VMEM((reach, channels), bf16),
        pltpu.VMEM((reach + rows, channels), f32),
        pltpu.VMEM((rows, n_tp * shared_gate.shape[1]), bf16),
        pltpu.VMEM((rows, n_tp * channels), bf16),
        pltpu.VMEM((n_tp, 1, rows), f32),
        pltpu.VMEM((2 * rows, expert_gate.shape[2]), bf16),
        pltpu.VMEM((n_z, 2 * rows, width), bf16),
        pltpu.VMEM((n_z, rows, width), bf16),
        pltpu.VMEM((n_z, rows, width), bf16),
        pltpu.VMEM((n_z, half, cols), bf16),
        pltpu.VMEM((n_z, half, cols), bf16),
        pltpu.VMEM((n_z, rows, cols), bf16),
        pltpu.VMEM((n_z, rows, cols), bf16),
        pltpu.VMEM((n_z, rows, cols), bf16),
        pltpu.VMEM((n_z, rows, cols), bf16),
        pltpu.VMEM((rows, cols), f32),
    ]
    dma = pltpu.SemaphoreType.DMA
    sems = (
        [dma((len(operands),))]
        + [dma((n_ep,))] * 2
        + [dma((n_z,))] * 24
        + [dma((2, 4))] * 2
        + [dma((3,))] * 2
        + [dma] * 2
    )
    return pl.pallas_call(
        lambda *refs: fused_kernel(n_ep, n_tp, *refs),
        out_shape=(
            jax.ShapeDtypeStruct((rows, cols), bf16),
            jax.ShapeDtypeStruct((rows, cols), bf16),
        ),
        in_specs=[pl.BlockSpec(memory_space=pltpu.HBM)] * len(operands),
        out_specs=(pl.BlockSpec(memory_space=pltpu.VMEM),) * 2,
        scratch_shapes=scratch + sems,
        compiler_params=pltpu.CompilerParams(
            collective_id=0, has_side_effects=True, vmem_limit_bytes=60 << 20
        ),
        name="fused",
    )(*operands)


def chosen(*arrays):
    route, expert_gate = arrays[8], arrays[10]
    experts = expert_gate.shape[0] * lax.axis_size("ep")
    capacity = 2 * route.shape[0] * route.shape[1] // experts
    square = lax.axis_size("tp") == 4 and lax.axis_size("ep") >= 6
    if capacity == route.shape[0] and expert_gate.shape[0] == 1 and square:
        return dense_on_device(*arrays)
    return on_device(*arrays)


def solution(mesh):
    return jax.shard_map(
        chosen,
        mesh=mesh,
        in_specs=(
            P("ep", None),
            P("ep", None),
            P(),
            P(),
            P(None, "tp"),
            P("tp"),
            P("tp"),
            P(None, "tp"),
            P("ep", None),
            P("ep", None),
            P("ep", None, "tp"),
            P("ep", None, "tp"),
            P("ep", "tp", None),
            P(None, "tp"),
            P(None, "tp"),
            P(None, "tp"),
        ),
        out_specs=(P("ep", "tp"), P("ep", "tp")),
        check_vma=False,
    )
```

```python
import jax
import jax.numpy as jnp
from jax import lax
from jax.experimental import pallas as pl
from jax.experimental.pallas import tpu as pltpu
from jax.sharding import PartitionSpec as P

epsilon = 1e-06
reach_rows = 15
window_widths = (2, 4, 8, 16)


def shifted(block, axis, distance):
    devices = range(lax.axis_size(axis))
    route = [(i - distance, i) for i in devices if i - distance in devices]
    return lax.ppermute(block, axis, route)


def row_norm(rows, gain):
    values = rows.astype(jnp.float32)
    scale = lax.rsqrt(jnp.mean(values * values, axis=-1, keepdims=True) + epsilon)
    return (values * scale * gain).astype(jnp.bfloat16)


def window_means(extended, position, group, n_rows):
    total = jnp.zeros((n_rows, extended.shape[1]), jnp.float32)
    result = jnp.zeros((n_rows, extended.shape[1]), jnp.float32)
    for lag in range(16):
        total = total + extended[reach_rows - lag : reach_rows - lag + n_rows]
        for index, width in enumerate(window_widths):
            if lag + 1 == width:
                count = jnp.minimum(position, float(width))[:, None]
                result = jnp.where(group[None, :] == index, total / count, result)
    return result - extended[reach_rows:]


def serve(sending, expert_gate, expert_up, expert_down):
    arrived = lax.all_to_all(sending, "ep", split_axis=0, concat_axis=0, tiled=True)
    gate = jnp.einsum("send,edf->senf", arrived, expert_gate, preferred_element_type=jnp.float32)
    upper = jnp.einsum("send,edf->senf", arrived, expert_up, preferred_element_type=jnp.float32)
    hidden = (jax.nn.silu(gate) * upper).astype(jnp.bfloat16)
    term = jnp.einsum("senf,efd->send", hidden, expert_down, preferred_element_type=jnp.float32)
    summed = lax.psum_scatter(term.astype(jnp.bfloat16), "tp", scatter_dimension=3, tiled=True)
    return lax.all_to_all(summed, "ep", split_axis=0, concat_axis=0, tiled=True)


def on_device(
    mix_input,
    expert_input,
    mix_gain,
    moe_gain,
    pool_in,
    pool_scale,
    pool_gain,
    pool_out,
    route,
    route_score,
    expert_gate,
    expert_up,
    expert_down,
    shared_gate,
    shared_up,
    shared_down,
):
    tok_rows = mix_input.shape[0]
    channels = pool_in.shape[1]
    pool_width = channels * lax.axis_size("tp")
    mix_norm = row_norm(mix_input, mix_gain)
    pool_input = jnp.dot(mix_norm, pool_in, preferred_element_type=jnp.float32).astype(jnp.bfloat16)
    before = shifted(pool_input[tok_rows - reach_rows :], "ep", 1)
    extended = jnp.concatenate([before, pool_input], axis=0).astype(jnp.float32)
    position = (lax.axis_index("ep") * tok_rows + jnp.arange(tok_rows, dtype=jnp.int32) + 1).astype(
        jnp.float32
    )
    channel_ids = lax.axis_index("tp") * channels + jnp.arange(channels, dtype=jnp.int32)
    group = channel_ids // (pool_width // 4)
    scaled = window_means(extended, position, group, tok_rows) * pool_scale
    squares = lax.psum(jnp.sum(scaled * scaled, axis=1), "tp")
    pooled_norm = (scaled * lax.rsqrt(squares / pool_width + epsilon)[:, None] * pool_gain).astype(
        jnp.bfloat16
    )
    moe_norm = row_norm(expert_input, moe_gain)
    shared_hidden = (
        jax.nn.silu(jnp.dot(moe_norm, shared_gate, preferred_element_type=jnp.float32))
        * jnp.dot(moe_norm, shared_up, preferred_element_type=jnp.float32)
    ).astype(jnp.bfloat16)
    pooled_all, shared_all = (
        lax.all_gather(pooled_norm, "tp", axis=1, tiled=True),
        lax.all_gather(shared_hidden, "tp", axis=1, tiled=True),
    )
    mix_out = jnp.dot(pooled_all, pool_out, preferred_element_type=jnp.float32).astype(jnp.bfloat16)
    shared_part = jnp.dot(shared_all, shared_down, preferred_element_type=jnp.float32)
    n_tok, top = route.shape
    local_experts = expert_gate.shape[0]
    experts = local_experts * lax.axis_size("ep")
    capacity = 2 * n_tok * top // experts
    flat_route = route.reshape(-1)
    table = (flat_route[:, None] == jnp.arange(experts, dtype=jnp.int32)[None, :]).astype(jnp.int32)
    ranks = jnp.sum((jnp.cumsum(table, axis=0) - table) * table, axis=1)
    slot = flat_route * capacity + ranks
    owner = (
        jnp.full((experts * capacity,), n_tok, jnp.int32)
        .at[slot]
        .set(jnp.arange(n_tok * top, dtype=jnp.int32) // top)
    )
    padded_rows = jnp.concatenate(
        [moe_norm, jnp.zeros((1, moe_norm.shape[1]), jnp.bfloat16)], axis=0
    )
    outgoing = padded_rows[owner].reshape(
        lax.axis_size("ep"), local_experts, capacity, moe_norm.shape[1]
    )
    middle = capacity // 2
    first = serve(outgoing[:, :, :middle], expert_gate, expert_up, expert_down)
    second = serve(outgoing[:, :, middle:], expert_gate, expert_up, expert_down)
    returned = jnp.concatenate([first, second], axis=2)
    back_rows = returned.reshape(experts * capacity, returned.shape[3])
    picked = back_rows[slot].reshape(n_tok, top, returned.shape[3]).astype(jnp.float32)
    weights = 2.5 * route_score / jnp.sum(route_score, axis=1, keepdims=True)
    routed = jnp.sum(picked * weights[:, :, None], axis=1)
    moe_out = (routed + shared_part).astype(jnp.bfloat16)
    return (mix_out, moe_out)


MESH = pl.DeviceIdType.MESH


def places():
    ep, tp = lax.axis_index("ep"), lax.axis_index("tp")
    z, core = ep // 2, ep % 2
    y, x = tp // 2, tp % 2
    return ep, tp, z, core, y * 2 + 1 - x, (1 - y) * 2 + x, (1 - y) * 2 + 1 - x


def aligned(start, size):
    return pl.ds(pl.multiple_of(start * size, size), size)


def fused_kernel(n_ep, n_tp, *refs):
    hbm, (mix_ref, moe_ref), rest = refs[:16], refs[16:18], refs[18:]
    (mi_h, ei_h, mg_h, eg_h, pi_h, ps_h, pg_h, po_h, rt_h, sc_h, wg_h, wu_h, wd_h, sg_h, su_h, sd_h) = hbm
    staged, rest = rest[:16], rest[16:]
    (mi, ei, mg, eg, pin, pscale, pgain, pout, rt, sc, wg, wu, wd, sg, su, sd) = staged
    (g, dense, mm, halo_s, halo_r, ext, sh_all, po_all, sq_all, hid) = rest[:10]
    (p, ca, s, bx, by, qx, qy, r, bz, o, so) = rest[10:21]
    l_sem = rest[21]
    (w_s, w_r, zu_s, zd_s, zf_s, z_r, e_s, e_r, d_s, d_r, gc_s, gc_r) = rest[22:34]
    (c_s, c_r, dx_s, dx_r, dy_s, dy_r, x_s, x_r, y_s, y_r, f_s, f_r, t_s, t_r, q_s, q_r, h_s, h_r) = rest[34:]
    ep, tp, z, core, xn, yn, dg = places()
    n_z = n_ep // 2
    rows, width = ei.shape
    cols = width // n_tp
    half = rows // 2
    f32, bf16 = jnp.float32, jnp.bfloat16
    other_core = z * 2 + 1 - core
    own_rows = aligned(ep, rows)
    low, high = pl.ds(0, half), pl.ds(half, half)

    loads = {}
    for number in (8, 9, 1, 3, 0, 2, 4, 13, 14, 5, 6, 10, 11, 12, 15, 7):
        loads[number] = pltpu.make_async_copy(hbm[number], staged[number], l_sem.at[number])
        loads[number].start()

    def send(src, dst, sem_s, sem_r, device):
        copy = pltpu.make_async_remote_copy(
            src_ref=src, dst_ref=dst, send_sem=sem_s, recv_sem=sem_r, device_id=device, device_id_type=MESH
        )
        copy.start()
        return copy

    halo = pltpu.make_async_remote_copy(
        src_ref=halo_s,
        dst_ref=halo_r,
        send_sem=h_s,
        recv_sem=h_r,
        device_id=((ep + 1) % n_ep, tp),
        device_id_type=MESH,
    )
    halo_r[...] = jnp.zeros_like(halo_r)
    peers = (xn, yn, dg)
    partners = [((ep + m) % n_ep, tp) for m in range(1, n_ep)] + [(ep, t) for t in peers]
    barrier = pltpu.get_barrier_semaphore()
    for partner in partners:
        pl.semaphore_signal(barrier, inc=1, device_id=partner, device_id_type=MESH)

    def norm_into(src, gain, dst, start):
        step = 16

        def some(index, carry):
            values = src[aligned(index, step), :].astype(f32)
            scale = lax.rsqrt(jnp.mean(values * values, axis=-1, keepdims=True) + epsilon)
            dst[pl.ds(pl.multiple_of(start + index * step, step), step), :] = (
                values * scale * gain[...]
            ).astype(bf16)
            return carry

        lax.fori_loop(0, rows // step, some, 0)

    with jax.named_scope("norm"):
        loads[8].wait()
        loads[9].wait()
        total_score = jnp.sum(sc[...], axis=0, keepdims=True)
        expert_ids = lax.broadcasted_iota(jnp.int32, (n_ep, rows), 0)
        mine = jnp.zeros((n_ep, rows), f32)
        for choice in range(rt.shape[0]):
            share = 2.5 * sc[choice : choice + 1, :] / total_score
            mine = mine + jnp.where(rt[choice : choice + 1, :] == expert_ids, share, 0.0)
        dense[ep] = mine
        loads[1].wait()
        loads[3].wait()
        norm_into(ei, eg, g, ep * rows)
    with jax.named_scope("greet"):
        pl.semaphore_wait(barrier, len(partners))
    w_copies = {}
    for m in range(1, n_ep):
        target = ((z + m // 2) % n_z) * 2 + (core + m) % 2
        w_copies[m] = send(dense.at[ep], dense.at[ep], w_s.at[m], w_r.at[ep], (target, tp))

    side = jnp.where(core == 0, tp % 2, tp // 2)
    facing = jnp.where(core == 0, xn, yn)
    wide = width // 2

    def z_piece(plane, part, columns):
        start = pl.multiple_of((plane * 2 + core) * rows + part * half, half)
        return g.at[pl.ds(start, half), aligned(columns, wide)]

    def remote(piece, sem_s, sem_r, device):
        return pltpu.make_async_remote_copy(
            src_ref=piece, dst_ref=piece, send_sem=sem_s, recv_sem=sem_r, device_id=device, device_id_type=MESH
        )

    upper_z, lower_z = jnp.minimum(z + 1, n_z - 1), jnp.maximum(z - 1, 0)
    for part in range(2):
        piece = z_piece(z, part, side)
        up = remote(piece, zu_s.at[part], z_r.at[z, part], (upper_z * 2 + core, tp))
        down_copy = remote(piece, zd_s.at[part], z_r.at[z, part], (lower_z * 2 + core, tp))
        pl.when(z < n_z - 1)(up.start)
        pl.when(z > 0)(down_copy.start)
    whole = g.at[own_rows, :]
    gc = {0: send(whole, whole, gc_s, gc_r, (other_core, tp))}

    distance = [jnp.maximum(z - q, q - z) for q in range(n_z)]
    planes = [0] * n_z
    for q in range(n_z):
        rank = 0
        for other in range(n_z):
            nearer = (distance[other] <= distance[q]) if other < q else (distance[other] < distance[q])
            rank = rank + jnp.where(nearer, 1, 0)
        for slot in range(n_z):
            planes[slot] = planes[slot] + jnp.where(rank == slot, q, 0)
    middle = (z > 0) & (z < n_z - 1)
    edge = jnp.logical_not(middle)

    def z_forward(slot, part):
        plane = planes[slot]
        target = jnp.where(plane < z, z + 1, z - 1)
        valid = (target >= 0) & (target < n_z)
        safe = jnp.maximum(jnp.minimum(target, n_z - 1), 0)
        piece = z_piece(plane, part, side)
        return valid, remote(piece, zf_s.at[slot, part], z_r.at[plane, part], (safe * 2 + core, tp))

    def e_copy(slot, part):
        piece = z_piece(planes[slot], part, side)
        return remote(piece, e_s.at[slot, part], e_r.at[slot, part], (ep, facing))

    def d_copy(slot, part, late):
        piece = z_piece(planes[slot], part, 1 - side if late else side)
        return remote(piece, d_s.at[slot, late, part], d_r.at[slot, late, part], (other_core, tp))

    def z_arrive(slot, part):
        with jax.named_scope(f"z_arrive{slot}{part}"):
            valid, forward = z_forward(slot, part)
            forward.wait_recv()
            pl.when(valid)(forward.start)
            e_copy(slot, part).start()
            d_copy(slot, part, 0).start()

    def e_arrive(slot, part):
        with jax.named_scope(f"e_arrive{slot}{part}"):
            e_copy(slot, part).wait_recv()
            d_copy(slot, part, 1).start()

    def gather_drain():
        for part in range(2):
            piece = z_piece(z, part, side)
            up = remote(piece, zu_s.at[part], z_r.at[z, part], (upper_z * 2 + core, tp))
            down_copy = remote(piece, zd_s.at[part], z_r.at[z, part], (lower_z * 2 + core, tp))
            pl.when(z < n_z - 1)(up.wait_send)
            pl.when(z > 0)(down_copy.wait_send)
            for slot in range(1, n_z):
                valid, forward = z_forward(slot, part)
                pl.when(valid)(forward.wait_send)
                e_copy(slot, part).wait_send()
                for late in range(2):
                    d_copy(slot, part, late).wait_send()

    with jax.named_scope("shared"):
        loads[13].wait()
        loads[14].wait()
        fs = sg.shape[1]
        tile = 256

        def shared_tile(index, carry):
            part = aligned(index, tile)
            gate = jnp.dot(g[own_rows, :], sg[:, part], preferred_element_type=f32)
            upper = jnp.dot(g[own_rows, :], su[:, part], preferred_element_type=f32)
            sh_all[:, pl.ds(pl.multiple_of(tp * fs + index * tile, tile), tile)] = (
                gate / (1.0 + jnp.exp(-gate)) * upper
            ).astype(bf16)
            return carry

        lax.fori_loop(0, fs // tile, shared_tile, 0)
    t_copies = {}

    def spread(kind, buffer):
        size = buffer.shape[1] // n_tp
        mine_slot = buffer.at[:, aligned(tp, size)]
        t_copies[kind, 0] = send(mine_slot, mine_slot, t_s.at[kind, 0], t_r.at[kind, 0], (ep, xn))
        t_copies[kind, 1] = send(mine_slot, mine_slot, t_s.at[kind, 1], t_r.at[kind, 1], (ep, yn))

    def spread_corner(kind, buffer):
        size = buffer.shape[1] // n_tp
        t_copies[kind, 0].wait_recv()
        part = buffer.at[low, aligned(xn, size)]
        t_copies[kind, 2] = send(part, part, t_s.at[kind, 2], t_r.at[kind, 2], (ep, yn))
        t_copies[kind, 1].wait_recv()
        part = buffer.at[high, aligned(yn, size)]
        t_copies[kind, 3] = send(part, part, t_s.at[kind, 3], t_r.at[kind, 3], (ep, xn))

    spread(0, sh_all)

    channels = pin.shape[1]
    reach = halo_s.shape[0]
    def pool_project():
        with jax.named_scope("pool_in"):
            loads[0].wait()
            loads[2].wait()
            norm_into(mi, mg, mm, 0)
            loads[4].wait()
            pooled_in = jnp.dot(mm[...], pin[...], preferred_element_type=f32).astype(bf16)
            halo_s[...] = pooled_in[rows - reach :]
            ext[reach:, :] = pooled_in.astype(f32)
            pl.when(ep < n_ep - 1)(halo.start)

    eye = lax.broadcasted_iota(jnp.int32, (rows, rows), 0) == lax.broadcasted_iota(
        jnp.int32, (rows, rows), 1
    )

    def window():
        pl.when(ep > 0)(halo.wait_recv)
        ext[:reach, :] = halo_r[...].astype(f32)
        position = (ep * rows + 1 + lax.broadcasted_iota(jnp.int32, (rows, 1), 0)).astype(f32)
        total = jnp.zeros((rows, channels), f32)
        result = jnp.zeros((rows, channels), f32)
        for lag in range(reach):
            total = total + ext[reach - lag : reach - lag + rows, :]
            for index, size in enumerate(window_widths):
                if lag + 1 == size:
                    count = jnp.minimum(position, float(size))
                    result = jnp.where(tp == index, total / count, result)
        loads[5].wait()
        loads[6].wait()
        scaled = (result - ext[reach:, :]) * pscale[...]
        squares = jnp.sum(scaled * scaled, axis=1, keepdims=True)
        sq_all[tp] = jnp.sum(jnp.where(eye, squares, 0.0), axis=0, keepdims=True)
        po_all[:, aligned(tp, channels)] = (scaled * pgain[...]).astype(bf16)

    c_copies, dx_copies, dy_copies, x_copies, y_copies, f_copies = {}, {}, {}, {}, {}, {}
    fe = wg.shape[1]

    def compute(k):
        plane = planes[k]
        with jax.named_scope(f"wait_over{k}"):
            if k == 0:
                gc[0].wait_recv()
            else:
                for late in range(2):
                    for part in range(2):
                        d_copy(k, part, late).wait_recv()
            for part in range(2):
                source = plane * 2 + part

                def arrive():
                    remote(dense.at[source], w_s.at[1], w_r.at[source], (other_core, tp)).wait_recv()

                if k == 0:
                    pl.when(core != part)(arrive)
                else:
                    arrive()
        with jax.named_scope(f"hidden{k}"):
            pair = aligned(plane, 2 * rows)
            factors = []
            for part in range(2):
                line = dense[plane * 2 + part, pl.ds(ep, 1), :]
                factors.append(jnp.sum(jnp.where(eye, line, 0.0), axis=1, keepdims=True))
            factor = jnp.concatenate(factors, axis=0)

            def tile_hidden(index, carry):
                part = aligned(index, tile)
                gate = jnp.dot(g[pair, :], wg[:, part], preferred_element_type=f32)
                upper = jnp.dot(g[pair, :], wu[:, part], preferred_element_type=f32)
                hid[:, part] = (gate / (1.0 + jnp.exp(-gate)) * upper * factor).astype(bf16)
                return carry

            lax.fori_loop(0, fe // tile, tile_hidden, 0)
        with jax.named_scope(f"down{k}"):

            def tile_down(index, carry):
                part = aligned(index, cols)
                p[k, :, part] = jnp.dot(hid[...], wd[:, part], preferred_element_type=f32).astype(bf16)
                return carry

            lax.fori_loop(0, width // cols, tile_down, 0)
            c_copies[k] = send(
                p.at[k, aligned(1 - core, rows), :], ca.at[k], c_s.at[k], c_r.at[k], (other_core, tp)
            )

    def first(k):
        with jax.named_scope(f"first{k}"):
            c_copies[k].wait_recv()
            s[k] = (p[k, aligned(core, rows), :].astype(f32) + ca[k].astype(f32)).astype(bf16)
            dx_copies[k] = send(
                s.at[k, low, aligned(dg, cols)], bx.at[k], dx_s.at[k], dx_r.at[k], (ep, xn)
            )
            dy_copies[k] = send(
                s.at[k, high, aligned(dg, cols)], by.at[k], dy_s.at[k], dy_r.at[k], (ep, yn)
            )

    def second(k):
        with jax.named_scope(f"second{k}"):
            dx_copies[k].wait_recv()
            s[k, low, aligned(yn, cols)] = (
                s[k, low, aligned(yn, cols)].astype(f32) + bx[k].astype(f32)
            ).astype(bf16)
            y_copies[k] = send(
                s.at[k, :, aligned(yn, cols)], qy.at[k], y_s.at[k], y_r.at[k], (ep, yn)
            )
            dy_copies[k].wait_recv()
            s[k, high, aligned(xn, cols)] = (
                s[k, high, aligned(xn, cols)].astype(f32) + by[k].astype(f32)
            ).astype(bf16)
            x_copies[k] = send(
                s.at[k, :, aligned(xn, cols)], qx.at[k], x_s.at[k], x_r.at[k], (ep, xn)
            )

    def third(k):
        with jax.named_scope(f"third{k}"):
            x_copies[k].wait_recv()
            y_copies[k].wait_recv()
            total = (
                s[k, :, aligned(tp, cols)].astype(f32) + qx[k].astype(f32) + qy[k].astype(f32)
            )
            if k == 0:
                o[...] = total
            else:
                r[k] = total.astype(bf16)
                f_copies[k] = send(
                    r.at[k], bz.at[z], f_s.at[k], f_r.at[z], (planes[k] * 2 + core, tp)
                )

    q_copies = []

    def finish_t():
        with jax.named_scope("epilogue"):
            for kind in range(2):
                t_copies[kind, 2].wait_recv()
                t_copies[kind, 3].wait_recv()
            for copy in q_copies:
                copy.wait()
            loads[15].wait()
            loads[7].wait()
            so[...] = jnp.dot(sh_all[...], sd[...], preferred_element_type=f32)
            mean = jnp.sum(sq_all[...], axis=0) / (channels * n_tp)
            inverse = lax.rsqrt(mean + epsilon)
            inverse = jnp.sum(jnp.where(eye, inverse, 0.0), axis=1, keepdims=True)
            mix_ref[...] = (
                jnp.dot(po_all[...], pout[...], preferred_element_type=f32) * inverse
            ).astype(bf16)

    def pooling():
        with jax.named_scope("window"):
            window()
        spread(1, po_all)
        for number, t in enumerate(peers):
            q_copies.append(send(sq_all.at[tp], sq_all.at[tp], q_s.at[number], q_r.at[number], (ep, t)))

    def turn(condition, *steps):
        def body():
            for step, slot in steps:
                for part in range(2):
                    step(slot, part)

        pl.when(condition)(body)

    last = n_z - 1
    with jax.named_scope("weights_wait"):
        for number in (10, 11, 12):
            loads[number].wait()
    compute(0)
    z_arrive(1, 0)
    pl.when(middle)(lambda: z_arrive(2, 0))
    z_arrive(1, 1)
    pl.when(middle)(lambda: z_arrive(2, 1))
    pool_project()
    first(0)
    e_arrive(1, 0)
    e_arrive(1, 1)
    with jax.named_scope("spread_corner"):
        spread_corner(0, sh_all)
    pooling()
    turn(middle, (e_arrive, 2))
    pl.when(middle)(lambda: z_arrive(3, 0))
    compute(1)
    turn(edge, (z_arrive, 2))
    pl.when(middle)(lambda: z_arrive(3, 1))
    second(0)
    first(1)
    pl.when(edge)(lambda: z_arrive(3, 0))
    turn(edge, (e_arrive, 2))
    with jax.named_scope("spread_corner"):
        spread_corner(1, po_all)
    pl.when(edge)(lambda: z_arrive(3, 1))
    turn(middle, (e_arrive, 3))
    compute(2)
    second(1)
    turn(edge, (e_arrive, 3))
    first(2)
    third(0)
    compute(3)
    second(2)
    third(1)
    first(3)
    finish_t()
    third(2)
    second(3)
    third(3)
    with jax.named_scope("final"):
        for k in range(1, n_z):
            source = planes[k]
            pltpu.make_async_remote_copy(
                src_ref=r.at[k],
                dst_ref=bz.at[source],
                send_sem=f_s.at[k],
                recv_sem=f_r.at[source],
                device_id=(source * 2 + core, tp),
                device_id_type=MESH,
            ).wait_recv()
            if k < last:
                o[...] += bz[source].astype(f32)
            else:
                moe_ref[...] = (o[...] + so[...] + bz[source].astype(f32)).astype(bf16)
    with jax.named_scope("drain"):
        pl.when(ep < n_ep - 1)(halo.wait_send)
        gather_drain()
        for group in (
            w_copies, gc, t_copies, c_copies, dx_copies, dy_copies, x_copies, y_copies, f_copies,
        ):
            for copy in group.values():
                copy.wait_send()


def dense_on_device(
    mix_input,
    expert_input,
    mix_gain,
    moe_gain,
    pool_in,
    pool_scale,
    pool_gain,
    pool_out,
    route,
    route_score,
    expert_gate,
    expert_up,
    expert_down,
    shared_gate,
    shared_up,
    shared_down,
):
    n_ep, n_tp = lax.axis_size("ep"), lax.axis_size("tp")
    n_z = n_ep // 2
    operands = (
        mix_input,
        expert_input,
        mix_gain.reshape(1, -1),
        moe_gain.reshape(1, -1),
        pool_in,
        pool_scale.reshape(1, -1),
        pool_gain.reshape(1, -1),
        pool_out,
        route.T,
        route_score.T,
        expert_gate[0],
        expert_up[0],
        expert_down[0],
        shared_gate,
        shared_up,
        shared_down,
    )
    rows, width = expert_input.shape
    cols = width // n_tp
    half = rows // 2
    channels = pool_in.shape[1]
    reach = reach_rows + 1
    f32, bf16 = jnp.float32, jnp.bfloat16
    scratch = [pltpu.VMEM(a.shape, a.dtype) for a in operands] + [
        pltpu.VMEM((n_ep * rows, width), bf16),
        pltpu.VMEM((n_ep, n_ep, rows), f32),
        pltpu.VMEM((rows, width), bf16),
        pltpu.VMEM((reach, channels), bf16),
        pltpu.VMEM((reach, channels), bf16),
        pltpu.VMEM((reach + rows, channels), f32),
        pltpu.VMEM((rows, n_tp * shared_gate.shape[1]), bf16),
        pltpu.VMEM((rows, n_tp * channels), bf16),
        pltpu.VMEM((n_tp, 1, rows), f32),
        pltpu.VMEM((2 * rows, expert_gate.shape[2]), bf16),
        pltpu.VMEM((n_z, 2 * rows, width), bf16),
        pltpu.VMEM((n_z, rows, width), bf16),
        pltpu.VMEM((n_z, rows, width), bf16),
        pltpu.VMEM((n_z, half, cols), bf16),
        pltpu.VMEM((n_z, half, cols), bf16),
        pltpu.VMEM((n_z, rows, cols), bf16),
        pltpu.VMEM((n_z, rows, cols), bf16),
        pltpu.VMEM((n_z, rows, cols), bf16),
        pltpu.VMEM((n_z, rows, cols), bf16),
        pltpu.VMEM((rows, cols), f32),
        pltpu.VMEM((rows, cols), f32),
    ]
    dma = pltpu.SemaphoreType.DMA
    sems = (
        [dma((len(operands),))]
        + [dma((n_ep,))] * 2
        + [dma((2,))] * 2
        + [dma((n_z, 2))] * 4
        + [dma((n_z, 2, 2))] * 2
        + [dma] * 2
        + [dma((n_z,))] * 12
        + [dma((2, 4))] * 2
        + [dma((3,))] * 2
        + [dma] * 2
    )
    return pl.pallas_call(
        lambda *refs: fused_kernel(n_ep, n_tp, *refs),
        out_shape=(
            pltpu.VMEM((rows, cols), bf16),
            pltpu.VMEM((rows, cols), bf16),
        ),
        in_specs=[pl.BlockSpec(memory_space=pltpu.HBM)] * len(operands),
        out_specs=(pl.BlockSpec(memory_space=pltpu.VMEM),) * 2,
        scratch_shapes=scratch + sems,
        compiler_params=pltpu.CompilerParams(
            collective_id=0, has_side_effects=True, vmem_limit_bytes=60 << 20
        ),
        name="fused",
    )(*operands)
def chosen(*arrays):
    route, expert_gate = arrays[8], arrays[10]
    experts = expert_gate.shape[0] * lax.axis_size("ep")
    capacity = 2 * route.shape[0] * route.shape[1] // experts
    square = lax.axis_size("tp") == 4 and lax.axis_size("ep") == 2 * lax.axis_size("tp")
    if capacity == route.shape[0] and expert_gate.shape[0] == 1 and square:
        return dense_on_device(*arrays)
    return on_device(*arrays)


def solution(mesh):
    return jax.shard_map(
        chosen,
        mesh=mesh,
        in_specs=(
            P("ep", None),
            P("ep", None),
            P(),
            P(),
            P(None, "tp"),
            P("tp"),
            P("tp"),
            P(None, "tp"),
            P("ep", None),
            P("ep", None),
            P("ep", None, "tp"),
            P("ep", None, "tp"),
            P("ep", "tp", None),
            P(None, "tp"),
            P(None, "tp"),
            P(None, "tp"),
        ),
        out_specs=(P("ep", "tp"), P("ep", "tp")),
        check_vma=False,
    )
```

```python
import jax
import jax.numpy as jnp
from jax import lax
from jax.experimental import pallas as pl
from jax.experimental.pallas import tpu as pltpu
from jax.sharding import PartitionSpec as P

epsilon = 1e-06
reach_rows = 15
window_widths = (2, 4, 8, 16)


def shifted(block, axis, distance):
    devices = range(lax.axis_size(axis))
    route = [(i - distance, i) for i in devices if i - distance in devices]
    return lax.ppermute(block, axis, route)


def row_norm(rows, gain):
    values = rows.astype(jnp.float32)
    scale = lax.rsqrt(jnp.mean(values * values, axis=-1, keepdims=True) + epsilon)
    return (values * scale * gain).astype(jnp.bfloat16)


def window_means(extended, position, group, n_rows):
    total = jnp.zeros((n_rows, extended.shape[1]), jnp.float32)
    result = jnp.zeros((n_rows, extended.shape[1]), jnp.float32)
    for lag in range(16):
        total = total + extended[reach_rows - lag : reach_rows - lag + n_rows]
        for index, width in enumerate(window_widths):
            if lag + 1 == width:
                count = jnp.minimum(position, float(width))[:, None]
                result = jnp.where(group[None, :] == index, total / count, result)
    return result - extended[reach_rows:]


def serve(sending, expert_gate, expert_up, expert_down):
    arrived = lax.all_to_all(sending, "ep", split_axis=0, concat_axis=0, tiled=True)
    gate = jnp.einsum("send,edf->senf", arrived, expert_gate, preferred_element_type=jnp.float32)
    upper = jnp.einsum("send,edf->senf", arrived, expert_up, preferred_element_type=jnp.float32)
    hidden = (jax.nn.silu(gate) * upper).astype(jnp.bfloat16)
    term = jnp.einsum("senf,efd->send", hidden, expert_down, preferred_element_type=jnp.float32)
    summed = lax.psum_scatter(term.astype(jnp.bfloat16), "tp", scatter_dimension=3, tiled=True)
    return lax.all_to_all(summed, "ep", split_axis=0, concat_axis=0, tiled=True)


def on_device(
    mix_input,
    expert_input,
    mix_gain,
    moe_gain,
    pool_in,
    pool_scale,
    pool_gain,
    pool_out,
    route,
    route_score,
    expert_gate,
    expert_up,
    expert_down,
    shared_gate,
    shared_up,
    shared_down,
):
    tok_rows = mix_input.shape[0]
    channels = pool_in.shape[1]
    pool_width = channels * lax.axis_size("tp")
    mix_norm = row_norm(mix_input, mix_gain)
    pool_input = jnp.dot(mix_norm, pool_in, preferred_element_type=jnp.float32).astype(jnp.bfloat16)
    before = shifted(pool_input[tok_rows - reach_rows :], "ep", 1)
    extended = jnp.concatenate([before, pool_input], axis=0).astype(jnp.float32)
    position = (lax.axis_index("ep") * tok_rows + jnp.arange(tok_rows, dtype=jnp.int32) + 1).astype(
        jnp.float32
    )
    channel_ids = lax.axis_index("tp") * channels + jnp.arange(channels, dtype=jnp.int32)
    group = channel_ids // (pool_width // 4)
    scaled = window_means(extended, position, group, tok_rows) * pool_scale
    squares = lax.psum(jnp.sum(scaled * scaled, axis=1), "tp")
    pooled_norm = (scaled * lax.rsqrt(squares / pool_width + epsilon)[:, None] * pool_gain).astype(
        jnp.bfloat16
    )
    moe_norm = row_norm(expert_input, moe_gain)
    shared_hidden = (
        jax.nn.silu(jnp.dot(moe_norm, shared_gate, preferred_element_type=jnp.float32))
        * jnp.dot(moe_norm, shared_up, preferred_element_type=jnp.float32)
    ).astype(jnp.bfloat16)
    pooled_all, shared_all = (
        lax.all_gather(pooled_norm, "tp", axis=1, tiled=True),
        lax.all_gather(shared_hidden, "tp", axis=1, tiled=True),
    )
    mix_out = jnp.dot(pooled_all, pool_out, preferred_element_type=jnp.float32).astype(jnp.bfloat16)
    shared_part = jnp.dot(shared_all, shared_down, preferred_element_type=jnp.float32)
    n_tok, top = route.shape
    local_experts = expert_gate.shape[0]
    experts = local_experts * lax.axis_size("ep")
    capacity = 2 * n_tok * top // experts
    flat_route = route.reshape(-1)
    table = (flat_route[:, None] == jnp.arange(experts, dtype=jnp.int32)[None, :]).astype(jnp.int32)
    ranks = jnp.sum((jnp.cumsum(table, axis=0) - table) * table, axis=1)
    slot = flat_route * capacity + ranks
    owner = (
        jnp.full((experts * capacity,), n_tok, jnp.int32)
        .at[slot]
        .set(jnp.arange(n_tok * top, dtype=jnp.int32) // top)
    )
    padded_rows = jnp.concatenate(
        [moe_norm, jnp.zeros((1, moe_norm.shape[1]), jnp.bfloat16)], axis=0
    )
    outgoing = padded_rows[owner].reshape(
        lax.axis_size("ep"), local_experts, capacity, moe_norm.shape[1]
    )
    middle = capacity // 2
    first = serve(outgoing[:, :, :middle], expert_gate, expert_up, expert_down)
    second = serve(outgoing[:, :, middle:], expert_gate, expert_up, expert_down)
    returned = jnp.concatenate([first, second], axis=2)
    back_rows = returned.reshape(experts * capacity, returned.shape[3])
    picked = back_rows[slot].reshape(n_tok, top, returned.shape[3]).astype(jnp.float32)
    weights = 2.5 * route_score / jnp.sum(route_score, axis=1, keepdims=True)
    routed = jnp.sum(picked * weights[:, :, None], axis=1)
    moe_out = (routed + shared_part).astype(jnp.bfloat16)
    return (mix_out, moe_out)


MESH = pl.DeviceIdType.MESH


def places():
    ep, tp = lax.axis_index("ep"), lax.axis_index("tp")
    z, core = ep // 2, ep % 2
    y, x = tp // 2, tp % 2
    return ep, tp, z, core, y * 2 + 1 - x, (1 - y) * 2 + x, (1 - y) * 2 + 1 - x


def aligned(start, size):
    return pl.ds(pl.multiple_of(start * size, size), size)


def fused_kernel(n_ep, n_tp, *refs):
    hbm, (mix_ref, moe_ref), rest = refs[:16], refs[16:18], refs[18:]
    (mi_h, ei_h, mg_h, eg_h, pi_h, ps_h, pg_h, po_h, rt_h, sc_h, wg_h, wu_h, wd_h, sg_h, su_h, sd_h) = hbm
    staged, rest = rest[:16], rest[16:]
    (mi, ei, mg, eg, pin, pscale, pgain, pout, rt, sc, wg, wu, wd, sg, su, sd) = staged
    (g, dense, mm, halo_s, halo_r, ext, sh_all, po_all, sq_all, hid) = rest[:10]
    (p, ca, s, bx, by, qx, qy, r, bz, o, so) = rest[10:21]
    pool = rest[21]
    ep, tp, z, core, xn, yn, dg = places()
    n_z = n_ep // 2
    last = n_z - 1
    counts = semaphore_counts(n_ep, n_tp)
    begins = {}
    for name in counts:
        begins[name] = sum(list(counts.values())[: list(counts).index(name)])

    def sem(name, index=0):
        return pool.at[begins[name] + index]

    rows, width = ei.shape
    cols = width // n_tp
    half = rows // 2
    f32, bf16 = jnp.float32, jnp.bfloat16
    other_core = z * 2 + 1 - core
    own_rows = aligned(ep, rows)
    low, high = pl.ds(0, half), pl.ds(half, half)

    loads = {}
    for number in (1, 3, 8, 9, 13, 14, 10, 11, 12, 0, 2, 4, 5, 6, 15, 7):
        loads[number] = pltpu.make_async_copy(hbm[number], staged[number], sem("load", number))
        loads[number].start()

    def send(src, dst, sem_s, sem_r, device):
        copy = pltpu.make_async_remote_copy(
            src_ref=src, dst_ref=dst, send_sem=sem_s, recv_sem=sem_r, device_id=device, device_id_type=MESH
        )
        copy.start()
        return copy

    halo = pltpu.make_async_remote_copy(
        src_ref=halo_s,
        dst_ref=halo_r,
        send_sem=sem("halo", 0),
        recv_sem=sem("halo", 1),
        device_id=((ep + 1) % n_ep, tp),
        device_id_type=MESH,
    )
    halo_r[...] = jnp.zeros_like(halo_r)
    peers = (xn, yn, dg)
    upper_z, lower_z = jnp.minimum(z + 1, n_z - 1), jnp.maximum(z - 1, 0)
    upper, lower = (upper_z * 2 + core, tp), (lower_z * 2 + core, tp)
    has_upper, has_lower = z < n_z - 1, z > 0
    barrier = pltpu.get_barrier_semaphore()

    def knock(partner):
        pl.semaphore_signal(barrier, inc=1, device_id=partner, device_id_type=MESH)

    for partner in ((other_core, tp), (ep, xn), (ep, yn)):
        knock(partner)
    pl.when(has_upper)(lambda: knock(upper))
    pl.when(has_lower)(lambda: knock(lower))

    def norm_into(src, gain, dst, start, first_row, n_rows):
        step = 16

        def some(index, carry):
            row = pl.multiple_of(first_row + index * step, step)
            values = src[pl.ds(row, step), :].astype(f32)
            scale = lax.rsqrt(jnp.mean(values * values, axis=-1, keepdims=True) + epsilon)
            dst[pl.ds(pl.multiple_of(start + row, step), step), :] = (
                values * scale * gain[...]
            ).astype(bf16)
            return carry

        lax.fori_loop(0, n_rows // step, some, 0)

    side = jnp.where(core == 0, tp % 2, tp // 2)
    facing = jnp.where(core == 0, xn, yn)
    wide = width // 2

    def z_piece(plane, part, columns):
        start = pl.multiple_of((plane * 2 + core) * rows + part * half, half)
        return g.at[pl.ds(start, half), aligned(columns, wide)]

    def remote(piece, sem_s, sem_r, device):
        return pltpu.make_async_remote_copy(
            src_ref=piece, dst_ref=piece, send_sem=sem_s, recv_sem=sem_r, device_id=device, device_id_type=MESH
        )

    def own_z(part):
        piece = z_piece(z, part, side)
        up = remote(piece, sem("own", 0), sem("z", z * 2 + part), upper)
        low_copy = remote(piece, sem("own", 1), sem("z", z * 2 + part), lower)
        return up, low_copy

    def own_w():
        up = remote(dense.at[ep], sem("w_own", 0), sem("w", ep), upper)
        low_copy = remote(dense.at[ep], sem("w_own", 1), sem("w", ep), lower)
        return up, low_copy

    def start_own(pair):
        pl.when(has_upper)(pair[0].start)
        pl.when(has_lower)(pair[1].start)

    with jax.named_scope("norm"):
        loads[1].wait()
        loads[3].wait()
        norm_into(ei, eg, g, ep * rows, 0, half)
    with jax.named_scope("greet"):
        pl.semaphore_wait(barrier, 3 + jnp.where(has_upper, 1, 0) + jnp.where(has_lower, 1, 0))
    with jax.named_scope("norm2"):
        start_own(own_z(0))
        norm_into(ei, eg, g, ep * rows, half, half)
        start_own(own_z(1))
    whole = g.at[own_rows, :]
    gc = {0: send(whole, whole, sem("sent"), sem("own_pair"), (other_core, tp))}
    with jax.named_scope("dense"):
        loads[8].wait()
        loads[9].wait()
        total_score = jnp.sum(sc[...], axis=0, keepdims=True)
        expert_ids = lax.broadcasted_iota(jnp.int32, (n_ep, rows), 0)
        mine = jnp.zeros((n_ep, rows), f32)
        for choice in range(rt.shape[0]):
            share = 2.5 * sc[choice : choice + 1, :] / total_score
            mine = mine + jnp.where(rt[choice : choice + 1, :] == expert_ids, share, 0.0)
        dense[ep] = mine
        start_own(own_w())
        send(dense.at[ep], dense.at[ep], sem("w_over"), sem("w", ep), (other_core, tp))

    inner = jnp.where(2 * z < n_z, 1, -1)
    distance = [2 * jnp.maximum(z - q, q - z) - jnp.where((q - z) * inner > 0, 1, 0) for q in range(n_z)]
    planes = [0] * n_z
    for q in range(n_z):
        rank = 0
        for other in range(n_z):
            nearer = (distance[other] <= distance[q]) if other < q else (distance[other] < distance[q])
            rank = rank + jnp.where(nearer, 1, 0)
        for slot in range(n_z):
            planes[slot] = planes[slot] + jnp.where(rank == slot, q, 0)
    middle = (z > 0) & (z < n_z - 1)
    edge = jnp.logical_not(middle)
    near, far = planes[n_z - 2], planes[n_z - 1]
    planes[n_z - 2] = jnp.where(middle, far, near)
    planes[n_z - 1] = jnp.where(middle, near, far)

    def z_forward(slot, part):
        plane = planes[slot]
        target = jnp.where(plane < z, z + 1, z - 1)
        valid = (target >= 0) & (target < n_z)
        safe = jnp.maximum(jnp.minimum(target, n_z - 1), 0)
        piece = z_piece(plane, part, side)
        return valid, remote(piece, sem("onward", slot - 1), sem("z", plane * 2 + part), (safe * 2 + core, tp))

    def w_forward(slot):
        plane = planes[slot]
        target = jnp.where(plane < z, z + 1, z - 1)
        safe = jnp.maximum(jnp.minimum(target, n_z - 1), 0)
        source = plane * 2 + core
        onward = remote(dense.at[source], sem("w_onward", slot - 1), sem("w", source), (safe * 2 + core, tp))
        over = remote(dense.at[source], sem("w_over"), sem("w", source), (other_core, tp))
        return onward, over

    def e_copy(slot, part):
        piece = z_piece(planes[slot], part, side)
        return remote(piece, sem("moved"), sem("e", (slot - 1) * 2 + part), (ep, facing))

    def d_copy(slot, part, late):
        piece = z_piece(planes[slot], part, 1 - side if late else side)
        return remote(piece, sem("moved"), sem("d", slot - 1), (other_core, tp))

    def z_arrive(slot, part):
        with jax.named_scope(f"z_arrive{slot}{part}"):
            valid, forward = z_forward(slot, part)
            forward.wait_recv()
            pl.when(valid)(forward.start)
            e_copy(slot, part).start()
            d_copy(slot, part, 0).start()
            if part == 1:
                onward, over = w_forward(slot)
                onward.wait_recv()
                pl.when(valid)(onward.start)
                over.start()

    def e_arrive(slot, part):
        with jax.named_scope(f"e_arrive{slot}{part}"):
            e_copy(slot, part).wait_recv()
            d_copy(slot, part, 1).start()

    def await_all(ref, name, index=0, received=False):
        copy = pltpu.make_async_remote_copy(
            src_ref=ref,
            dst_ref=ref,
            send_sem=sem(name, index),
            recv_sem=sem(name, index),
            device_id=(other_core, tp),
            device_id_type=MESH,
        )
        if received:
            copy.wait_recv()
        else:
            copy.wait_send()

    def block_of(n_rows, n_columns):
        return g.at[pl.ds(0, n_rows), pl.ds(0, n_columns)]

    def gather_drain():
        def own_sent(number):
            await_all(block_of(rows, wide), "own", number)
            await_all(dense.at[0], "w_own", number)

        def onward_sent(slot):
            await_all(block_of(rows, wide), "onward", slot - 1)
            await_all(dense.at[0], "w_onward", slot - 1)

        pl.when(has_upper)(lambda: own_sent(0))
        pl.when(has_lower)(lambda: own_sent(1))
        for slot in range(1, n_z):
            valid, _ = z_forward(slot, 0)
            pl.when(valid)(lambda: onward_sent(slot))
        await_all(dense.at[pl.ds(0, n_z)], "w_over")

    with jax.named_scope("shared"):
        loads[13].wait()
        loads[14].wait()
        fs = sg.shape[1]
        tile = 256

        def shared_tile(index, carry):
            part = aligned(index, tile)
            gate = jnp.dot(g[own_rows, :], sg[:, part], preferred_element_type=f32)
            upper = jnp.dot(g[own_rows, :], su[:, part], preferred_element_type=f32)
            sh_all[:, pl.ds(pl.multiple_of(tp * fs + index * tile, tile), tile)] = (
                gate / (1.0 + jnp.exp(-gate)) * upper
            ).astype(bf16)
            return carry

        lax.fori_loop(0, fs // tile, shared_tile, 0)
    t_copies = {}

    def spread(kind, buffer):
        size = buffer.shape[1] // n_tp
        mine_slot = buffer.at[:, aligned(tp, size)]
        t_copies[kind, 0] = send(mine_slot, mine_slot, sem("sent"), sem("t", kind * 3), (ep, xn))
        t_copies[kind, 1] = send(mine_slot, mine_slot, sem("sent"), sem("t", kind * 3 + 1), (ep, yn))

    def spread_corner(kind, buffer):
        size = buffer.shape[1] // n_tp
        t_copies[kind, 0].wait_recv()
        part = buffer.at[low, aligned(xn, size)]
        t_copies[kind, 2] = send(part, part, sem("sent"), sem("t", kind * 3 + 2), (ep, yn))
        t_copies[kind, 1].wait_recv()
        part = buffer.at[high, aligned(yn, size)]
        t_copies[kind, 3] = send(part, part, sem("sent"), sem("t", kind * 3 + 2), (ep, xn))

    def corner_arrived(kind, buffer):
        size = buffer.shape[1] // n_tp
        await_all(buffer.at[:, pl.ds(0, size)], "t", kind * 3 + 2, True)

    spread(0, sh_all)

    channels = pin.shape[1]
    reach = halo_s.shape[0]
    def pool_project():
        with jax.named_scope("pool_in"):
            loads[0].wait()
            loads[2].wait()
            norm_into(mi, mg, mm, 0, 0, rows)
            loads[4].wait()
            pooled_in = jnp.dot(mm[...], pin[...], preferred_element_type=f32).astype(bf16)
            halo_s[...] = pooled_in[rows - reach :]
            ext[reach:, :] = pooled_in.astype(f32)
            pl.when(ep < n_ep - 1)(halo.start)

    eye = lax.broadcasted_iota(jnp.int32, (rows, rows), 0) == lax.broadcasted_iota(
        jnp.int32, (rows, rows), 1
    )

    def window():
        pl.when(ep > 0)(halo.wait_recv)
        ext[:reach, :] = halo_r[...].astype(f32)
        position = (ep * rows + 1 + lax.broadcasted_iota(jnp.int32, (rows, 1), 0)).astype(f32)
        total = jnp.zeros((rows, channels), f32)
        result = jnp.zeros((rows, channels), f32)
        for lag in range(reach):
            total = total + ext[reach - lag : reach - lag + rows, :]
            for index, size in enumerate(window_widths):
                if lag + 1 == size:
                    count = jnp.minimum(position, float(size))
                    result = jnp.where(tp == index, total / count, result)
        loads[5].wait()
        loads[6].wait()
        scaled = (result - ext[reach:, :]) * pscale[...]
        squares = jnp.sum(scaled * scaled, axis=1, keepdims=True)
        sq_all[tp] = jnp.sum(jnp.where(eye, squares, 0.0), axis=0, keepdims=True)
        po_all[:, aligned(tp, channels)] = (scaled * pgain[...]).astype(bf16)

    c_copies, dx_copies, dy_copies, x_copies, y_copies, f_copies = {}, {}, {}, {}, {}, {}
    fe = wg.shape[1]

    def hidden(k):
        plane = planes[k]
        with jax.named_scope(f"wait_over{k}"):
            if k == 0:
                gc[0].wait_recv()
            else:
                await_all(block_of(rows, width), "d", k - 1, True)
            source = plane * 2 + 1 - core
            remote(dense.at[source], sem("w_own", 0), sem("w", source), (other_core, tp)).wait_recv()
        with jax.named_scope(f"hidden{k}"):
            pair = aligned(plane, 2 * rows)
            factors = []
            for part in range(2):
                line = dense[plane * 2 + part, pl.ds(ep, 1), :]
                factors.append(jnp.sum(jnp.where(eye, line, 0.0), axis=1, keepdims=True))
            factor = jnp.concatenate(factors, axis=0)
            for index in range(fe // tile):
                part = pl.ds(index * tile, tile)
                gate = jnp.dot(g[pair, :], wg[:, part], preferred_element_type=f32)
                upper = jnp.dot(g[pair, :], wu[:, part], preferred_element_type=f32)
                hid[:, part] = (gate / (1.0 + jnp.exp(-gate)) * upper * factor).astype(bf16)

    quarters = (dg, yn, xn, tp)

    def down(k):
        with jax.named_scope(f"down{k}"):
            if k < last:
                for index in range(n_tp):
                    part = pl.ds(index * cols, cols)
                    p[k, :, part] = jnp.dot(hid[...], wd[:, part], preferred_element_type=f32).astype(bf16)
            if k < last:
                c_copies[k, 0] = send(
                    p.at[k, aligned(1 - core, rows), :], ca.at[k], sem("sent"), sem("c", k), (other_core, tp)
                )
            else:
                for number, quarter in enumerate(quarters):
                    part = aligned(quarter, cols)
                    p[k, :, part] = jnp.dot(hid[...], wd[:, part], preferred_element_type=f32).astype(bf16)
                    c_copies[k, number] = send(
                        p.at[k, aligned(1 - core, rows), part],
                        ca.at[k, :, part],
                        sem("sent"),
                        sem("c", k + number),
                        (other_core, tp),
                    )

    def cuts(k):
        return 2 if k in (0, last) else 1

    def place(k, cut):
        return sum(cuts(other) for other in range(k)) + cut

    def strip(k, quarter, cut):
        size = cols // cuts(k)
        return pl.ds(pl.multiple_of(quarter * cols + cut * size, size), size)

    def local_strip(k, cut):
        size = cols // cuts(k)
        return pl.ds(cut * size, size)

    def merge(k, number):
        if (k, number) in c_copies:
            c_copies[k, number].wait_recv()
        part = aligned(quarters[number], cols)
        s[k, :, part] = (
            p[k, aligned(core, rows), part].astype(f32) + ca[k, :, part].astype(f32)
        ).astype(bf16)

    def first(k):
        with jax.named_scope(f"first{k}"):
            merge(k, 0)
            for cut in range(cuts(k)):
                here, there = strip(k, dg, cut), local_strip(k, cut)
                dx_copies[k, cut] = send(
                    s.at[k, low, here], bx.at[k, :, there], sem("moved"), sem("dx", place(k, cut)), (ep, xn)
                )
                dy_copies[k, cut] = send(
                    s.at[k, high, here], by.at[k, :, there], sem("moved"), sem("dy", place(k, cut)), (ep, yn)
                )
            for number in range(1, len(quarters)):
                merge(k, number)

    def second(k):
        with jax.named_scope(f"second{k}"):
            for cut in range(cuts(k)):
                there = local_strip(k, cut)
                here = strip(k, yn, cut)
                dx_copies[k, cut].wait_recv()
                s[k, low, here] = (
                    s[k, low, here].astype(f32) + bx[k, :, there].astype(f32)
                ).astype(bf16)
                y_copies[k, cut] = send(
                    s.at[k, :, here], qy.at[k, :, there], sem("moved"), sem("xy", place(k, cut)), (ep, yn)
                )
                here = strip(k, xn, cut)
                dy_copies[k, cut].wait_recv()
                s[k, high, here] = (
                    s[k, high, here].astype(f32) + by[k, :, there].astype(f32)
                ).astype(bf16)
                x_copies[k, cut] = send(
                    s.at[k, :, here], qx.at[k, :, there], sem("moved"), sem("xy", place(k, cut)), (ep, xn)
                )

    def third(k):
        with jax.named_scope(f"third{k}"):
            for cut in range(cuts(k)):
                there = local_strip(k, cut)
                await_all(block_of(2 * rows, cols // cuts(k)), "xy", place(k, cut), True)
                total = (
                    s[k, :, strip(k, tp, cut)].astype(f32)
                    + qx[k, :, there].astype(f32)
                    + qy[k, :, there].astype(f32)
                )
                if k == 0:
                    o[:, there] = total
                else:
                    r[k, :, there] = total.astype(bf16)
                    f_copies[k, cut] = send(
                        r.at[k, :, there],
                        bz.at[z, :, there],
                        sem("sent"),
                        sem("f", z),
                        (planes[k] * 2 + core, tp),
                    )


    def finish_t():
        with jax.named_scope("epilogue"):
            corner_arrived(1, po_all)
            await_all(sq_all.at[pl.ds(0, n_tp - 1)], "squares", 1, True)
            loads[15].wait()
            loads[7].wait()
            so[...] = jnp.dot(sh_all[...], sd[...], preferred_element_type=f32)
            mean = jnp.sum(sq_all[...], axis=0) / (channels * n_tp)
            inverse = lax.rsqrt(mean + epsilon)
            inverse = jnp.sum(jnp.where(eye, inverse, 0.0), axis=1, keepdims=True)
            mix_ref[...] = (
                jnp.dot(po_all[...], pout[...], preferred_element_type=f32) * inverse
            ).astype(bf16)

    def spread_squares(number):
        line = sq_all.at[tp]
        send(line, line, sem("squares", 0), sem("squares", 1), (ep, peers[number]))

    def pooling():
        with jax.named_scope("window"):
            window()
        spread(1, po_all)
        for number in range(2):
            spread_squares(number)

    with jax.named_scope("weights_wait"):
        for number in (10, 11, 12):
            loads[number].wait()
    def on_edge(step, *which):
        pl.when(edge)(lambda: step(*which))

    def on_middle(step, *which):
        pl.when(middle)(lambda: step(*which))

    hidden(0)
    down(0)
    z_arrive(1, 0)
    on_middle(z_arrive, 3, 0)
    pool_project()
    z_arrive(1, 1)
    on_middle(z_arrive, 3, 1)
    with jax.named_scope("spread_corner"):
        spread_corner(0, sh_all)
    e_arrive(1, 0)
    e_arrive(1, 1)
    pooling()
    z_arrive(2, 0)
    hidden(1)
    down(1)
    z_arrive(2, 1)
    first(1)
    with jax.named_scope("spread_corner"):
        spread_corner(1, po_all)
        corner_arrived(0, sh_all)
        spread_squares(2)
    e_arrive(2, 0)
    on_edge(z_arrive, 3, 0)
    second(1)
    e_arrive(2, 1)
    hidden(2)
    on_edge(z_arrive, 3, 1)
    down(2)
    e_arrive(3, 0)
    first(2)
    third(1)
    e_arrive(3, 1)
    hidden(3)
    second(2)
    down(3)
    first(3)
    first(0)
    third(2)
    second(3)
    second(0)
    finish_t()
    third(3)
    third(0)
    with jax.named_scope("final"):
        o[...] += so[...]
        for k in range(1, n_z):
            source = planes[k]
            pltpu.make_async_remote_copy(
                src_ref=r.at[k],
                dst_ref=bz.at[source],
                send_sem=sem("sent"),
                recv_sem=sem("f", source),
                device_id=(source * 2 + core, tp),
                device_id_type=MESH,
            ).wait_recv()
            if k < last:
                o[...] += bz[source].astype(f32)
            else:
                moe_ref[...] = (o[...] + bz[source].astype(f32)).astype(bf16)
    with jax.named_scope("drain"):
        pl.when(ep < n_ep - 1)(halo.wait_send)
        gather_drain()
        await_all(sq_all.at[pl.ds(0, n_tp - 1)], "squares", 0)
        shared_rows = 3 * half * (sh_all.shape[1] + po_all.shape[1]) // (n_tp * width) * 2
        await_all(block_of((n_z + 1) * rows + last * rows // n_tp + shared_rows, width), "sent")
        await_all(block_of(3 * half * last + 3 * half * n_z * 2 // n_tp, width), "moved")


def semaphore_counts(n_ep, n_tp):
    n_z = n_ep // 2
    return {
        "load": 16, "own": 2, "w_own": 2, "onward": n_z - 1, "w_onward": n_z - 1, "w_over": 1,
        "sent": 1, "moved": 1, "z": 2 * n_z, "w": n_ep, "own_pair": 1, "e": 2 * (n_z - 1),
        "d": n_z - 1, "c": n_z - 1 + n_tp, "dx": n_z + 2, "dy": n_z + 2, "xy": n_z + 2, "f": n_z,
        "t": 6, "squares": 2, "halo": 2,
    }


def dense_on_device(
    mix_input,
    expert_input,
    mix_gain,
    moe_gain,
    pool_in,
    pool_scale,
    pool_gain,
    pool_out,
    route,
    route_score,
    expert_gate,
    expert_up,
    expert_down,
    shared_gate,
    shared_up,
    shared_down,
):
    n_ep, n_tp = lax.axis_size("ep"), lax.axis_size("tp")
    n_z = n_ep // 2
    operands = (
        mix_input,
        expert_input,
        mix_gain.reshape(1, -1),
        moe_gain.reshape(1, -1),
        pool_in,
        pool_scale.reshape(1, -1),
        pool_gain.reshape(1, -1),
        pool_out,
        route.T,
        route_score.T,
        expert_gate[0],
        expert_up[0],
        expert_down[0],
        shared_gate,
        shared_up,
        shared_down,
    )
    rows, width = expert_input.shape
    cols = width // n_tp
    half = rows // 2
    channels = pool_in.shape[1]
    reach = reach_rows + 1
    f32, bf16 = jnp.float32, jnp.bfloat16
    scratch = [pltpu.VMEM(a.shape, a.dtype) for a in operands] + [
        pltpu.VMEM((n_ep * rows, width), bf16),
        pltpu.VMEM((n_ep, n_ep, rows), f32),
        pltpu.VMEM((rows, width), bf16),
        pltpu.VMEM((reach, channels), bf16),
        pltpu.VMEM((reach, channels), bf16),
        pltpu.VMEM((reach + rows, channels), f32),
        pltpu.VMEM((rows, n_tp * shared_gate.shape[1]), bf16),
        pltpu.VMEM((rows, n_tp * channels), bf16),
        pltpu.VMEM((n_tp, 1, rows), f32),
        pltpu.VMEM((2 * rows, expert_gate.shape[2]), bf16),
        pltpu.VMEM((n_z, 2 * rows, width), bf16),
        pltpu.VMEM((n_z, rows, width), bf16),
        pltpu.VMEM((n_z, rows, width), bf16),
        pltpu.VMEM((n_z, half, cols), bf16),
        pltpu.VMEM((n_z, half, cols), bf16),
        pltpu.VMEM((n_z, rows, cols), bf16),
        pltpu.VMEM((n_z, rows, cols), bf16),
        pltpu.VMEM((n_z, rows, cols), bf16),
        pltpu.VMEM((n_z, rows, cols), bf16),
        pltpu.VMEM((rows, cols), f32),
        pltpu.VMEM((rows, cols), f32),
    ]
    sems = [pltpu.SemaphoreType.DMA((sum(semaphore_counts(n_ep, n_tp).values()),))]
    return pl.pallas_call(
        lambda *refs: fused_kernel(n_ep, n_tp, *refs),
        out_shape=(
            pltpu.VMEM((rows, cols), bf16),
            pltpu.VMEM((rows, cols), bf16),
        ),
        in_specs=[pl.BlockSpec(memory_space=pltpu.HBM)] * len(operands),
        out_specs=(pl.BlockSpec(memory_space=pltpu.VMEM),) * 2,
        scratch_shapes=scratch + sems,
        compiler_params=pltpu.CompilerParams(
            collective_id=0, has_side_effects=True, vmem_limit_bytes=60 << 20
        ),
        name="fused",
    )(*operands)
def chosen(*arrays):
    route, expert_gate = arrays[8], arrays[10]
    experts = expert_gate.shape[0] * lax.axis_size("ep")
    capacity = 2 * route.shape[0] * route.shape[1] // experts
    square = lax.axis_size("tp") == 4 and lax.axis_size("ep") == 2 * lax.axis_size("tp")
    if capacity == route.shape[0] and expert_gate.shape[0] == 1 and square:
        return dense_on_device(*arrays)
    return on_device(*arrays)


def solution(mesh):
    return jax.shard_map(
        chosen,
        mesh=mesh,
        in_specs=(
            P("ep", None),
            P("ep", None),
            P(),
            P(),
            P(None, "tp"),
            P("tp"),
            P("tp"),
            P(None, "tp"),
            P("ep", None),
            P("ep", None),
            P("ep", None, "tp"),
            P("ep", None, "tp"),
            P("ep", "tp", None),
            P(None, "tp"),
            P(None, "tp"),
            P(None, "tp"),
        ),
        out_specs=(P("ep", "tp"), P("ep", "tp")),
        check_vma=False,
    )
```

```python
import jax
import jax.numpy as jnp
from jax import lax
from jax.experimental import pallas as pl
from jax.experimental.pallas import tpu as pltpu
from jax.sharding import PartitionSpec as P

epsilon = 1e-06
reach_rows = 15
window_widths = (2, 4, 8, 16)


def shifted(block, axis, distance):
    devices = range(lax.axis_size(axis))
    route = [(i - distance, i) for i in devices if i - distance in devices]
    return lax.ppermute(block, axis, route)


def row_norm(rows, gain):
    values = rows.astype(jnp.float32)
    scale = lax.rsqrt(jnp.mean(values * values, axis=-1, keepdims=True) + epsilon)
    return (values * scale * gain).astype(jnp.bfloat16)


def window_means(extended, position, group, n_rows):
    total = jnp.zeros((n_rows, extended.shape[1]), jnp.float32)
    result = jnp.zeros((n_rows, extended.shape[1]), jnp.float32)
    for lag in range(16):
        total = total + extended[reach_rows - lag : reach_rows - lag + n_rows]
        for index, width in enumerate(window_widths):
            if lag + 1 == width:
                count = jnp.minimum(position, float(width))[:, None]
                result = jnp.where(group[None, :] == index, total / count, result)
    return result - extended[reach_rows:]


def serve(sending, expert_gate, expert_up, expert_down):
    arrived = lax.all_to_all(sending, "ep", split_axis=0, concat_axis=0, tiled=True)
    gate = jnp.einsum("send,edf->senf", arrived, expert_gate, preferred_element_type=jnp.float32)
    upper = jnp.einsum("send,edf->senf", arrived, expert_up, preferred_element_type=jnp.float32)
    hidden = (jax.nn.silu(gate) * upper).astype(jnp.bfloat16)
    term = jnp.einsum("senf,efd->send", hidden, expert_down, preferred_element_type=jnp.float32)
    summed = lax.psum_scatter(term.astype(jnp.bfloat16), "tp", scatter_dimension=3, tiled=True)
    return lax.all_to_all(summed, "ep", split_axis=0, concat_axis=0, tiled=True)


def on_device(
    mix_input,
    expert_input,
    mix_gain,
    moe_gain,
    pool_in,
    pool_scale,
    pool_gain,
    pool_out,
    route,
    route_score,
    expert_gate,
    expert_up,
    expert_down,
    shared_gate,
    shared_up,
    shared_down,
):
    tok_rows = mix_input.shape[0]
    channels = pool_in.shape[1]
    pool_width = channels * lax.axis_size("tp")
    mix_norm = row_norm(mix_input, mix_gain)
    pool_input = jnp.dot(mix_norm, pool_in, preferred_element_type=jnp.float32).astype(jnp.bfloat16)
    before = shifted(pool_input[tok_rows - reach_rows :], "ep", 1)
    extended = jnp.concatenate([before, pool_input], axis=0).astype(jnp.float32)
    position = (lax.axis_index("ep") * tok_rows + jnp.arange(tok_rows, dtype=jnp.int32) + 1).astype(
        jnp.float32
    )
    channel_ids = lax.axis_index("tp") * channels + jnp.arange(channels, dtype=jnp.int32)
    group = channel_ids // (pool_width // 4)
    scaled = window_means(extended, position, group, tok_rows) * pool_scale
    squares = lax.psum(jnp.sum(scaled * scaled, axis=1), "tp")
    pooled_norm = (scaled * lax.rsqrt(squares / pool_width + epsilon)[:, None] * pool_gain).astype(
        jnp.bfloat16
    )
    moe_norm = row_norm(expert_input, moe_gain)
    shared_hidden = (
        jax.nn.silu(jnp.dot(moe_norm, shared_gate, preferred_element_type=jnp.float32))
        * jnp.dot(moe_norm, shared_up, preferred_element_type=jnp.float32)
    ).astype(jnp.bfloat16)
    pooled_all, shared_all = (
        lax.all_gather(pooled_norm, "tp", axis=1, tiled=True),
        lax.all_gather(shared_hidden, "tp", axis=1, tiled=True),
    )
    mix_out = jnp.dot(pooled_all, pool_out, preferred_element_type=jnp.float32).astype(jnp.bfloat16)
    shared_part = jnp.dot(shared_all, shared_down, preferred_element_type=jnp.float32)
    n_tok, top = route.shape
    local_experts = expert_gate.shape[0]
    experts = local_experts * lax.axis_size("ep")
    capacity = 2 * n_tok * top // experts
    flat_route = route.reshape(-1)
    table = (flat_route[:, None] == jnp.arange(experts, dtype=jnp.int32)[None, :]).astype(jnp.int32)
    ranks = jnp.sum((jnp.cumsum(table, axis=0) - table) * table, axis=1)
    slot = flat_route * capacity + ranks
    owner = (
        jnp.full((experts * capacity,), n_tok, jnp.int32)
        .at[slot]
        .set(jnp.arange(n_tok * top, dtype=jnp.int32) // top)
    )
    padded_rows = jnp.concatenate(
        [moe_norm, jnp.zeros((1, moe_norm.shape[1]), jnp.bfloat16)], axis=0
    )
    outgoing = padded_rows[owner].reshape(
        lax.axis_size("ep"), local_experts, capacity, moe_norm.shape[1]
    )
    middle = capacity // 2
    first = serve(outgoing[:, :, :middle], expert_gate, expert_up, expert_down)
    second = serve(outgoing[:, :, middle:], expert_gate, expert_up, expert_down)
    returned = jnp.concatenate([first, second], axis=2)
    back_rows = returned.reshape(experts * capacity, returned.shape[3])
    picked = back_rows[slot].reshape(n_tok, top, returned.shape[3]).astype(jnp.float32)
    weights = 2.5 * route_score / jnp.sum(route_score, axis=1, keepdims=True)
    routed = jnp.sum(picked * weights[:, :, None], axis=1)
    moe_out = (routed + shared_part).astype(jnp.bfloat16)
    return (mix_out, moe_out)


MESH = pl.DeviceIdType.MESH


def places():
    ep, tp = lax.axis_index("ep"), lax.axis_index("tp")
    z, core = ep // 2, ep % 2
    y, x = tp // 2, tp % 2
    return ep, tp, z, core, y * 2 + 1 - x, (1 - y) * 2 + x, (1 - y) * 2 + 1 - x


def aligned(start, size):
    return pl.ds(pl.multiple_of(start * size, size), size)


def fused_kernel(n_ep, n_tp, *refs):
    hbm, out_ref, rest = refs[:16], refs[16], refs[17:]
    (mi_h, ei_h, mg_h, eg_h, pi_h, ps_h, pg_h, po_h, rt_h, sc_h, wg_h, wu_h, wd_h, sg_h, su_h, sd_h) = hbm
    staged, rest = rest[:16], rest[16:]
    (mi, ei, mg, eg, pin, pscale, pgain, pout, rt, sc, wg, wu, wd, sg, su, sd) = staged
    (g, dense, mm, halo_s, halo_r, ext, sh_all, po_all, sq_all, hid) = rest[:10]
    (p, ca, s, bx, by, qx, qy, r, bz, o, so, lifted) = rest[10:22]
    pool = rest[22]
    ep, tp, z, core, xn, yn, dg = places()
    n_z = n_ep // 2
    last = n_z - 1
    counts = semaphore_counts(n_ep, n_tp)
    begins = {}
    for name in counts:
        begins[name] = sum(list(counts.values())[: list(counts).index(name)])

    def sem(name, index=0):
        return pool.at[begins[name] + index]

    rows, width = ei.shape
    cols = width // n_tp
    half = rows // 2
    f32, bf16 = jnp.float32, jnp.bfloat16
    other_core = z * 2 + 1 - core
    own_rows = aligned(ep, rows)
    low, high = pl.ds(0, half), pl.ds(half, half)

    loads = {}
    for number in (1, 3, 8, 9, 13, 14, 10, 11, 12, 0, 2, 4, 5, 6, 15, 7):
        loads[number] = pltpu.make_async_copy(hbm[number], staged[number], sem("load", number))
        loads[number].start()

    def send(src, dst, sem_s, sem_r, device):
        copy = pltpu.make_async_remote_copy(
            src_ref=src, dst_ref=dst, send_sem=sem_s, recv_sem=sem_r, device_id=device, device_id_type=MESH
        )
        copy.start()
        return copy

    halo = pltpu.make_async_remote_copy(
        src_ref=halo_s,
        dst_ref=halo_r,
        send_sem=sem("halo", 0),
        recv_sem=sem("halo", 1),
        device_id=((ep + 1) % n_ep, tp),
        device_id_type=MESH,
    )
    halo_r[...] = jnp.zeros_like(halo_r)
    lifted[...] = jnp.zeros_like(lifted)
    peers = (xn, yn, dg)
    upper_z, lower_z = jnp.minimum(z + 1, n_z - 1), jnp.maximum(z - 1, 0)
    upper, lower = (upper_z * 2 + core, tp), (lower_z * 2 + core, tp)
    has_upper, has_lower = z < n_z - 1, z > 0
    barrier = pltpu.get_barrier_semaphore()

    def knock(partner):
        pl.semaphore_signal(barrier, inc=1, device_id=partner, device_id_type=MESH)

    for partner in ((other_core, tp), (ep, xn), (ep, yn)):
        knock(partner)
    pl.when(has_upper)(lambda: knock(upper))
    pl.when(has_lower)(lambda: knock(lower))

    def norm_into(src, gain, dst, start, first_row, n_rows):
        step = 16

        def some(index, carry):
            row = pl.multiple_of(first_row + index * step, step)
            values = src[pl.ds(row, step), :].astype(f32)
            scale = lax.rsqrt(jnp.mean(values * values, axis=-1, keepdims=True) + epsilon)
            dst[pl.ds(pl.multiple_of(start + row, step), step), :] = (
                values * scale * gain[...]
            ).astype(bf16)
            return carry

        lax.fori_loop(0, n_rows // step, some, 0)

    side = jnp.where(core == 0, tp % 2, tp // 2)
    facing = jnp.where(core == 0, xn, yn)
    wide = width // 2

    def z_piece(plane, part, columns):
        start = pl.multiple_of((plane * 2 + core) * rows + part * half, half)
        return g.at[pl.ds(start, half), aligned(columns, wide)]

    def remote(piece, sem_s, sem_r, device):
        return pltpu.make_async_remote_copy(
            src_ref=piece, dst_ref=piece, send_sem=sem_s, recv_sem=sem_r, device_id=device, device_id_type=MESH
        )

    middle = has_upper & has_lower
    edge = jnp.logical_not(middle)

    def own_z(part):
        piece = z_piece(z, part, side)
        up = remote(piece, sem("own", 0), sem("z", z * 2 + part), upper)
        low_copy = remote(piece, sem("own", 1), sem("z", z * 2 + part), lower)
        return up, low_copy

    def start_own_z(part):
        up, low_copy = own_z(part)
        pl.when(middle)(up.start)
        pl.when(middle)(low_copy.start)
        inner = jnp.where(has_upper, upper_z, lower_z)
        straight = remote(
            z_piece(z, part, side), sem("own", 0), sem("z", z * 2 + part), (inner * 2 + core, tp)
        )
        pl.when(edge)(straight.start)

    def start_rest():
        inner = jnp.where(has_upper, upper_z, lower_z)
        for part in range(2):
            rest_copy = remote(
                z_piece(z, part, 1 - side),
                sem("own", 0),
                sem("e", (last - 1) * 2 + part),
                (inner * 2 + core, tp),
            )
            pl.when(edge)(rest_copy.start)

    def own_w():
        up = remote(dense.at[ep], sem("w_own", 0), sem("w", ep), upper)
        low_copy = remote(dense.at[ep], sem("w_own", 1), sem("w", ep), lower)
        return up, low_copy

    def start_own(pair):
        pl.when(has_upper)(pair[0].start)
        pl.when(has_lower)(pair[1].start)

    with jax.named_scope("norm"):
        loads[1].wait()
        loads[3].wait()
        norm_into(ei, eg, g, ep * rows, 0, half)
    with jax.named_scope("greet"):
        pl.semaphore_wait(barrier, 3 + jnp.where(has_upper, 1, 0) + jnp.where(has_lower, 1, 0))
    with jax.named_scope("norm2"):
        start_own_z(0)
        norm_into(ei, eg, g, ep * rows, half, half)
        start_own_z(1)
    whole = g.at[own_rows, :]
    gc = {0: send(whole, whole, sem("sent"), sem("own_pair"), (other_core, tp))}
    with jax.named_scope("dense"):
        loads[8].wait()
        loads[9].wait()
        total_score = jnp.sum(sc[...], axis=0, keepdims=True)
        expert_ids = lax.broadcasted_iota(jnp.int32, (n_ep, rows), 0)
        mine = jnp.zeros((n_ep, rows), f32)
        for choice in range(rt.shape[0]):
            share = 2.5 * sc[choice : choice + 1, :] / total_score
            mine = mine + jnp.where(rt[choice : choice + 1, :] == expert_ids, share, 0.0)
        dense[ep] = mine
        start_own(own_w())
        send(dense.at[ep], dense.at[ep], sem("w_over"), sem("w", ep), (other_core, tp))

    inner = jnp.where(2 * z < n_z, 1, -1)
    distance = [2 * jnp.maximum(z - q, q - z) - jnp.where((q - z) * inner > 0, 1, 0) for q in range(n_z)]
    planes = [0] * n_z
    for q in range(n_z):
        rank = 0
        for other in range(n_z):
            nearer = (distance[other] <= distance[q]) if other < q else (distance[other] < distance[q])
            rank = rank + jnp.where(nearer, 1, 0)
        for slot in range(n_z):
            planes[slot] = planes[slot] + jnp.where(rank == slot, q, 0)
    near, far = planes[n_z - 2], planes[n_z - 1]
    planes[n_z - 2] = jnp.where(middle, far, near)
    planes[n_z - 1] = jnp.where(middle, near, far)

    def z_forward(slot, part):
        plane = planes[slot]
        target = jnp.where(plane < z, z + 1, z - 1)
        valid = (target >= 0) & (target < n_z)
        safe = jnp.maximum(jnp.minimum(target, n_z - 1), 0)
        piece = z_piece(plane, part, side)
        return valid, remote(piece, sem("onward", slot - 1), sem("z", plane * 2 + part), (safe * 2 + core, tp))

    def w_forward(slot):
        plane = planes[slot]
        target = jnp.where(plane < z, z + 1, z - 1)
        safe = jnp.maximum(jnp.minimum(target, n_z - 1), 0)
        source = plane * 2 + core
        onward = remote(dense.at[source], sem("w_onward", slot - 1), sem("w", source), (safe * 2 + core, tp))
        over = remote(dense.at[source], sem("w_over"), sem("w", source), (other_core, tp))
        return onward, over

    def e_copy(slot, part):
        piece = z_piece(planes[slot], part, side)
        return remote(piece, sem("moved"), sem("e", (slot - 1) * 2 + part), (ep, facing))

    def d_copy(slot, part, late):
        piece = z_piece(planes[slot], part, 1 - side if late else side)
        return remote(piece, sem("moved"), sem("d", slot - 1), (other_core, tp))

    def z_arrive(slot, part, exchange=True):
        with jax.named_scope(f"z_arrive{slot}{part}"):
            valid, forward = z_forward(slot, part)
            forward.wait_recv()
            pl.when(valid)(forward.start)
            if exchange:
                e_copy(slot, part).start()
            d_copy(slot, part, 0).start()
            if part == 1:
                onward, over = w_forward(slot)
                onward.wait_recv()
                pl.when(valid)(onward.start)
                over.start()

    def full_arrive(slot, part):
        z_arrive(slot, part, False)

    def e_arrive(slot, part):
        with jax.named_scope(f"e_arrive{slot}{part}"):
            e_copy(slot, part).wait_recv()
            d_copy(slot, part, 1).start()

    def await_all(ref, name, index=0, received=False):
        copy = pltpu.make_async_remote_copy(
            src_ref=ref,
            dst_ref=ref,
            send_sem=sem(name, index),
            recv_sem=sem(name, index),
            device_id=(other_core, tp),
            device_id_type=MESH,
        )
        if received:
            copy.wait_recv()
        else:
            copy.wait_send()

    def block_of(n_rows, n_columns):
        return g.at[pl.ds(0, n_rows), pl.ds(0, n_columns)]

    def gather_drain():
        def own_sent(number):
            await_all(dense.at[0], "w_own", number)

        def onward_sent(slot):
            await_all(block_of(rows, wide), "onward", slot - 1)
            await_all(dense.at[0], "w_onward", slot - 1)

        pl.when(middle)(lambda: await_all(block_of(rows, wide), "own", 0))
        pl.when(middle)(lambda: await_all(block_of(rows, wide), "own", 1))
        pl.when(edge)(lambda: await_all(block_of(rows, width), "own", 0))
        pl.when(has_upper)(lambda: own_sent(0))
        pl.when(has_lower)(lambda: own_sent(1))
        for slot in range(1, n_z):
            valid, _ = z_forward(slot, 0)
            pl.when(valid)(lambda: onward_sent(slot))
        await_all(dense.at[pl.ds(0, n_z)], "w_over")

    with jax.named_scope("shared"):
        loads[13].wait()
        loads[14].wait()
        fs = sg.shape[1]
        tile = 256

        def shared_tile(index, carry):
            part = aligned(index, tile)
            gate = jnp.dot(g[own_rows, :], sg[:, part], preferred_element_type=f32)
            upper = jnp.dot(g[own_rows, :], su[:, part], preferred_element_type=f32)
            sh_all[:, pl.ds(pl.multiple_of(tp * fs + index * tile, tile), tile)] = (
                gate / (1.0 + jnp.exp(-gate)) * upper
            ).astype(bf16)
            return carry

        lax.fori_loop(0, fs // tile, shared_tile, 0)
    t_copies = {}

    def spread(kind, buffer):
        size = buffer.shape[1] // n_tp
        mine_slot = buffer.at[:, aligned(tp, size)]
        t_copies[kind, 0] = send(mine_slot, mine_slot, sem("sent"), sem("t", kind * 4), (ep, xn))
        t_copies[kind, 1] = send(mine_slot, mine_slot, sem("sent"), sem("t", kind * 4 + 1), (ep, yn))

    def spread_corner(kind, buffer):
        size = buffer.shape[1] // n_tp
        t_copies[kind, 0].wait_recv()
        part = buffer.at[low, aligned(xn, size)]
        t_copies[kind, 2] = send(part, part, sem("sent"), sem("t", kind * 4 + 2), (ep, yn))
        t_copies[kind, 1].wait_recv()
        part = buffer.at[high, aligned(yn, size)]
        t_copies[kind, 3] = send(part, part, sem("sent"), sem("t", kind * 4 + 3), (ep, xn))

    def corner_arrived(kind, buffer):
        size = buffer.shape[1] // n_tp
        for number in (2, 3):
            await_all(buffer.at[low, pl.ds(0, size)], "t", kind * 4 + number, True)

    spread(0, sh_all)

    channels = pin.shape[1]
    reach = halo_s.shape[0]
    def pool_project():
        with jax.named_scope("pool_in"):
            loads[0].wait()
            loads[2].wait()
            norm_into(mi, mg, mm, 0, 0, rows)
            loads[4].wait()
            pooled_in = jnp.dot(mm[...], pin[...], preferred_element_type=f32).astype(bf16)
            halo_s[...] = pooled_in[rows - reach :]
            ext[reach:, :] = pooled_in.astype(f32)
            pl.when(ep < n_ep - 1)(halo.start)

    eye = lax.broadcasted_iota(jnp.int32, (rows, rows), 0) == lax.broadcasted_iota(
        jnp.int32, (rows, rows), 1
    )

    def window():
        pl.when(ep > 0)(halo.wait_recv)
        ext[:reach, :] = halo_r[...].astype(f32)
        position = (ep * rows + 1 + lax.broadcasted_iota(jnp.int32, (rows, 1), 0)).astype(f32)
        total = jnp.zeros((rows, channels), f32)
        result = jnp.zeros((rows, channels), f32)
        for lag in range(reach):
            total = total + ext[reach - lag : reach - lag + rows, :]
            for index, size in enumerate(window_widths):
                if lag + 1 == size:
                    count = jnp.minimum(position, float(size))
                    result = jnp.where(tp == index, total / count, result)
        loads[5].wait()
        loads[6].wait()
        scaled = (result - ext[reach:, :]) * pscale[...]
        squares = jnp.sum(scaled * scaled, axis=1, keepdims=True)
        sq_all[tp] = jnp.sum(jnp.where(eye, squares, 0.0), axis=0, keepdims=True)
        po_all[:, aligned(tp, channels)] = (scaled * pgain[...]).astype(bf16)

    c_copies = {}
    fe = wg.shape[1]

    def hidden(k):
        plane = planes[k]
        with jax.named_scope(f"wait_over{k}"):
            if k == 0:
                gc[0].wait_recv()
            else:
                await_all(block_of(rows, width), "d", k - 1, True)
            source = plane * 2 + 1 - core
            remote(dense.at[source], sem("w_own", 0), sem("w", source), (other_core, tp)).wait_recv()
        with jax.named_scope(f"hidden{k}"):
            pair = aligned(plane, 2 * rows)
            factors = []
            for part in range(2):
                line = dense[plane * 2 + part, pl.ds(ep, 1), :]
                factors.append(jnp.sum(jnp.where(eye, line, 0.0), axis=1, keepdims=True))
            factor = jnp.concatenate(factors, axis=0)
            for index in range(fe // tile):
                part = pl.ds(index * tile, tile)
                gate = jnp.dot(g[pair, :], wg[:, part], preferred_element_type=f32)
                upper = jnp.dot(g[pair, :], wu[:, part], preferred_element_type=f32)
                hid[:, part] = (gate / (1.0 + jnp.exp(-gate)) * upper * factor).astype(bf16)

    quarters = (dg, yn, xn, tp)

    def down(k):
        with jax.named_scope(f"down{k}"):
            if k < last:
                for index in range(n_tp):
                    part = pl.ds(index * cols, cols)
                    p[k, :, part] = jnp.dot(hid[...], wd[:, part], preferred_element_type=f32).astype(bf16)
            if k < last:
                c_copies[k, 0] = send(
                    p.at[k, aligned(1 - core, rows), :], ca.at[k], sem("sent"), sem("c", k), (other_core, tp)
                )
            else:
                for number, quarter in enumerate(quarters):
                    part = aligned(quarter, cols)
                    p[k, :, part] = jnp.dot(hid[...], wd[:, part], preferred_element_type=f32).astype(bf16)
                    c_copies[k, number] = send(
                        p.at[k, aligned(1 - core, rows), part],
                        ca.at[k, :, part],
                        sem("sent"),
                        sem("c", k + number),
                        (other_core, tp),
                    )

    def cuts(k):
        return 2 if k in (0, last) else 1

    def place(k, cut):
        return sum(cuts(other) for other in range(k)) + cut

    def strip(k, quarter, cut):
        size = cols // cuts(k)
        return pl.ds(pl.multiple_of(quarter * cols + cut * size, size), size)

    def local_strip(k, cut):
        size = cols // cuts(k)
        return pl.ds(cut * size, size)

    def merge(k, number):
        if (k, number) in c_copies:
            c_copies[k, number].wait_recv()
        part = aligned(quarters[number], cols)
        own, theirs = p[k, aligned(core, rows), part].astype(f32), ca[k, :, part].astype(f32)
        if k == 0:
            own = own + lifted[:, part].astype(f32)
        s[k, :, part] = (own + theirs).astype(bf16)

    def first(k):
        with jax.named_scope(f"first{k}"):
            merge(k, 0)
            for cut in range(cuts(k)):
                here, there = strip(k, dg, cut), local_strip(k, cut)
                send(
                    s.at[k, low, here], bx.at[k, :, there], sem("moved"), sem("dx", place(k, cut)), (ep, xn)
                )
                send(
                    s.at[k, high, here], by.at[k, :, there], sem("moved"), sem("dy", place(k, cut)), (ep, yn)
                )
            for number in range(1, len(quarters)):
                merge(k, number)

    def lift():
        inner = jnp.where(has_upper, upper_z, lower_z)
        return pltpu.make_async_remote_copy(
            src_ref=s.at[1],
            dst_ref=lifted,
            send_sem=sem("lift", 0),
            recv_sem=sem("lift", 1),
            device_id=(inner * 2 + core, tp),
            device_id_type=MESH,
        )

    def lift_start():
        with jax.named_scope("lift"):
            for number in range(len(quarters)):
                merge(1, number)
            lift().start()

    def lift_arrive():
        with jax.named_scope("lift_wait"):
            lift().wait_recv()

    def second(k):
        with jax.named_scope(f"second{k}"):
            for cut in range(cuts(k)):
                there = local_strip(k, cut)
                here = strip(k, yn, cut)
                await_all(bx.at[k, :, there], "dx", place(k, cut), True)
                s[k, low, here] = (
                    s[k, low, here].astype(f32) + bx[k, :, there].astype(f32)
                ).astype(bf16)
                send(
                    s.at[k, :, here], qy.at[k, :, there], sem("moved"), sem("xy", place(k, cut)), (ep, yn)
                )
                here = strip(k, xn, cut)
                await_all(by.at[k, :, there], "dy", place(k, cut), True)
                s[k, high, here] = (
                    s[k, high, here].astype(f32) + by[k, :, there].astype(f32)
                ).astype(bf16)
                send(
                    s.at[k, :, here], qx.at[k, :, there], sem("moved"), sem("xy", place(k, cut)), (ep, xn)
                )

    def third(k):
        with jax.named_scope(f"third{k}"):
            for cut in range(cuts(k)):
                there = local_strip(k, cut)
                await_all(block_of(2 * rows, cols // cuts(k)), "xy", place(k, cut), True)
                total = (
                    s[k, :, strip(k, tp, cut)].astype(f32)
                    + qx[k, :, there].astype(f32)
                    + qy[k, :, there].astype(f32)
                )
                if k == 0:
                    o[:, there] = total
                else:
                    r[k, :, there] = total.astype(bf16)
                    send(
                        r.at[k, :, there],
                        bz.at[z, :, there],
                        sem("sent"),
                        sem("f", z),
                        (planes[k] * 2 + core, tp),
                    )


    def finish_t():
        with jax.named_scope("epilogue"):
            corner_arrived(1, po_all)
            await_all(sq_all.at[pl.ds(0, n_tp - 1)], "squares", 1, True)
            loads[15].wait()
            loads[7].wait()
            so[...] = jnp.dot(sh_all[...], sd[...], preferred_element_type=f32)
            mean = jnp.sum(sq_all[...], axis=0) / (channels * n_tp)
            inverse = lax.rsqrt(mean + epsilon)
            inverse = jnp.sum(jnp.where(eye, inverse, 0.0), axis=1, keepdims=True)
            out_ref[:rows] = (
                jnp.dot(po_all[...], pout[...], preferred_element_type=f32) * inverse
            ).astype(bf16)

    def spread_squares(number):
        line = sq_all.at[tp]
        send(line, line, sem("squares", 0), sem("squares", 1), (ep, peers[number]))

    def pooling():
        with jax.named_scope("window"):
            window()
        spread(1, po_all)
        for number in range(2):
            spread_squares(number)

    with jax.named_scope("weights_wait"):
        for number in (10, 11, 12):
            loads[number].wait()
    def on_edge(step, *which):
        pl.when(edge)(lambda: step(*which))

    def on_middle(step, *which):
        pl.when(middle)(lambda: step(*which))

    hidden(0)
    down(0)
    z_arrive(1, 0)
    start_rest()
    on_middle(full_arrive, 3, 0)
    pool_project()
    z_arrive(1, 1)
    on_middle(full_arrive, 3, 1)
    with jax.named_scope("spread_corner"):
        spread_corner(0, sh_all)
    e_arrive(1, 0)
    e_arrive(1, 1)
    pooling()
    z_arrive(2, 0)
    hidden(1)
    z_arrive(2, 1)
    down(1)
    on_edge(lift_start)
    on_middle(first, 1)
    with jax.named_scope("spread_corner"):
        spread_corner(1, po_all)
        for number in (2, 3):
            t_copies[0, number].wait_recv()
        spread_squares(2)
    e_arrive(2, 0)
    on_edge(z_arrive, 3, 0)
    on_edge(z_arrive, 3, 1)
    on_middle(second, 1)
    e_arrive(2, 1)
    hidden(2)
    down(2)
    e_arrive(3, 0)
    first(2)
    e_arrive(3, 1)
    hidden(3)
    second(2)
    on_middle(third, 1)
    down(3)
    first(3)
    on_middle(lift_arrive)
    first(0)
    third(2)
    second(3)
    second(0)
    finish_t()
    third(3)
    third(0)
    with jax.named_scope("final"):
        o[...] += so[...]

        def collect(k):
            source = planes[k]
            pltpu.make_async_remote_copy(
                src_ref=r.at[k],
                dst_ref=bz.at[source],
                send_sem=sem("sent"),
                recv_sem=sem("f", source),
                device_id=(source * 2 + core, tp),
                device_id_type=MESH,
            ).wait_recv()
            o[...] += bz[source].astype(f32)

        for k in range(1, last):
            collect(k)
        pl.when(edge)(lambda: collect(last))
        out_ref[rows:] = o[...].astype(bf16)
    with jax.named_scope("drain"):
        pl.when(ep < n_ep - 1)(halo.wait_send)
        gather_drain()
        await_all(sq_all.at[pl.ds(0, n_tp - 1)], "squares", 0)
        shared_rows = 3 * half * (sh_all.shape[1] + po_all.shape[1]) // (n_tp * width) * 2
        sent_rows = (n_z + 1) * rows + last * rows // n_tp + shared_rows
        moved_rows = 3 * half * last + 3 * half * n_z * 2 // n_tp

        def middle_sent():
            await_all(block_of(sent_rows, width), "sent")
            await_all(block_of(moved_rows - half, width), "moved")

        def edge_sent():
            await_all(block_of(sent_rows - rows // n_tp, width), "sent")
            await_all(block_of(moved_rows - 3 * half * 2 // n_tp, width), "moved")
            await_all(lifted, "lift", 0)

        pl.when(middle)(middle_sent)
        pl.when(edge)(edge_sent)


def semaphore_counts(n_ep, n_tp):
    n_z = n_ep // 2
    return {
        "load": 16, "own": 2, "w_own": 2, "onward": n_z - 1, "w_onward": n_z - 1, "w_over": 1,
        "sent": 1, "moved": 1, "z": 2 * n_z, "w": n_ep, "own_pair": 1, "e": 2 * (n_z - 1),
        "d": n_z - 1, "c": n_z - 1 + n_tp, "dx": n_z + 2, "dy": n_z + 2, "xy": n_z + 2, "f": n_z,
        "t": 8, "squares": 2, "halo": 2, "lift": 2,
    }


def dense_on_device(
    mix_input,
    expert_input,
    mix_gain,
    moe_gain,
    pool_in,
    pool_scale,
    pool_gain,
    pool_out,
    route,
    route_score,
    expert_gate,
    expert_up,
    expert_down,
    shared_gate,
    shared_up,
    shared_down,
):
    n_ep, n_tp = lax.axis_size("ep"), lax.axis_size("tp")
    n_z = n_ep // 2
    operands = (
        mix_input,
        expert_input,
        mix_gain.reshape(1, -1),
        moe_gain.reshape(1, -1),
        pool_in,
        pool_scale.reshape(1, -1),
        pool_gain.reshape(1, -1),
        pool_out,
        route.T,
        route_score.T,
        expert_gate[0],
        expert_up[0],
        expert_down[0],
        shared_gate,
        shared_up,
        shared_down,
    )
    rows, width = expert_input.shape
    cols = width // n_tp
    half = rows // 2
    channels = pool_in.shape[1]
    reach = reach_rows + 1
    f32, bf16 = jnp.float32, jnp.bfloat16
    scratch = [pltpu.VMEM(a.shape, a.dtype) for a in operands] + [
        pltpu.VMEM((n_ep * rows, width), bf16),
        pltpu.VMEM((n_ep, n_ep, rows), f32),
        pltpu.VMEM((rows, width), bf16),
        pltpu.VMEM((reach, channels), bf16),
        pltpu.VMEM((reach, channels), bf16),
        pltpu.VMEM((reach + rows, channels), f32),
        pltpu.VMEM((rows, n_tp * shared_gate.shape[1]), bf16),
        pltpu.VMEM((rows, n_tp * channels), bf16),
        pltpu.VMEM((n_tp, 1, rows), f32),
        pltpu.VMEM((2 * rows, expert_gate.shape[2]), bf16),
        pltpu.VMEM((n_z, 2 * rows, width), bf16),
        pltpu.VMEM((n_z, rows, width), bf16),
        pltpu.VMEM((n_z, rows, width), bf16),
        pltpu.VMEM((n_z, half, cols), bf16),
        pltpu.VMEM((n_z, half, cols), bf16),
        pltpu.VMEM((n_z, rows, cols), bf16),
        pltpu.VMEM((n_z, rows, cols), bf16),
        pltpu.VMEM((n_z, rows, cols), bf16),
        pltpu.VMEM((n_z, rows, cols), bf16),
        pltpu.VMEM((rows, cols), f32),
        pltpu.VMEM((rows, cols), f32),
        pltpu.VMEM((rows, width), bf16),
    ]
    sems = [pltpu.SemaphoreType.DMA((sum(semaphore_counts(n_ep, n_tp).values()),))]
    both = pl.pallas_call(
        lambda *refs: fused_kernel(n_ep, n_tp, *refs),
        out_shape=pltpu.VMEM((2 * rows, cols), bf16),
        in_specs=[pl.BlockSpec(memory_space=pltpu.HBM)] * len(operands),
        out_specs=pl.BlockSpec(memory_space=pltpu.VMEM),
        scratch_shapes=scratch + sems,
        compiler_params=pltpu.CompilerParams(
            collective_id=0, has_side_effects=True, vmem_limit_bytes=60 << 20
        ),
        name="fused",
    )(*operands)
    return both[:rows], both[rows:]
def chosen(*arrays):
    route, expert_gate = arrays[8], arrays[10]
    experts = expert_gate.shape[0] * lax.axis_size("ep")
    capacity = 2 * route.shape[0] * route.shape[1] // experts
    square = lax.axis_size("tp") == 4 and lax.axis_size("ep") == 2 * lax.axis_size("tp")
    if capacity == route.shape[0] and expert_gate.shape[0] == 1 and square:
        return dense_on_device(*arrays)
    return on_device(*arrays)


def solution(mesh):
    return jax.shard_map(
        chosen,
        mesh=mesh,
        in_specs=(
            P("ep", None),
            P("ep", None),
            P(),
            P(),
            P(None, "tp"),
            P("tp"),
            P("tp"),
            P(None, "tp"),
            P("ep", None),
            P("ep", None),
            P("ep", None, "tp"),
            P("ep", None, "tp"),
            P("ep", "tp", None),
            P(None, "tp"),
            P(None, "tp"),
            P(None, "tp"),
        ),
        out_specs=(P("ep", "tp"), P("ep", "tp")),
        check_vma=False,
    )
```

```python
import jax
import jax.numpy as jnp
from jax import lax
from jax.experimental import pallas as pl
from jax.experimental.pallas import tpu as pltpu
from jax.sharding import PartitionSpec as P

epsilon = 1e-06
reach_rows = 15
window_widths = (2, 4, 8, 16)


def shifted(block, axis, distance):
    devices = range(lax.axis_size(axis))
    route = [(i - distance, i) for i in devices if i - distance in devices]
    return lax.ppermute(block, axis, route)


def row_norm(rows, gain):
    values = rows.astype(jnp.float32)
    scale = lax.rsqrt(jnp.mean(values * values, axis=-1, keepdims=True) + epsilon)
    return (values * scale * gain).astype(jnp.bfloat16)


def window_means(extended, position, group, n_rows):
    total = jnp.zeros((n_rows, extended.shape[1]), jnp.float32)
    result = jnp.zeros((n_rows, extended.shape[1]), jnp.float32)
    for lag in range(16):
        total = total + extended[reach_rows - lag : reach_rows - lag + n_rows]
        for index, width in enumerate(window_widths):
            if lag + 1 == width:
                count = jnp.minimum(position, float(width))[:, None]
                result = jnp.where(group[None, :] == index, total / count, result)
    return result - extended[reach_rows:]


def serve(sending, expert_gate, expert_up, expert_down):
    arrived = lax.all_to_all(sending, "ep", split_axis=0, concat_axis=0, tiled=True)
    gate = jnp.einsum("send,edf->senf", arrived, expert_gate, preferred_element_type=jnp.float32)
    upper = jnp.einsum("send,edf->senf", arrived, expert_up, preferred_element_type=jnp.float32)
    hidden = (jax.nn.silu(gate) * upper).astype(jnp.bfloat16)
    term = jnp.einsum("senf,efd->send", hidden, expert_down, preferred_element_type=jnp.float32)
    summed = lax.psum_scatter(term.astype(jnp.bfloat16), "tp", scatter_dimension=3, tiled=True)
    return lax.all_to_all(summed, "ep", split_axis=0, concat_axis=0, tiled=True)


def on_device(
    mix_input,
    expert_input,
    mix_gain,
    moe_gain,
    pool_in,
    pool_scale,
    pool_gain,
    pool_out,
    route,
    route_score,
    expert_gate,
    expert_up,
    expert_down,
    shared_gate,
    shared_up,
    shared_down,
):
    tok_rows = mix_input.shape[0]
    channels = pool_in.shape[1]
    pool_width = channels * lax.axis_size("tp")
    mix_norm = row_norm(mix_input, mix_gain)
    pool_input = jnp.dot(mix_norm, pool_in, preferred_element_type=jnp.float32).astype(jnp.bfloat16)
    before = shifted(pool_input[tok_rows - reach_rows :], "ep", 1)
    extended = jnp.concatenate([before, pool_input], axis=0).astype(jnp.float32)
    position = (lax.axis_index("ep") * tok_rows + jnp.arange(tok_rows, dtype=jnp.int32) + 1).astype(
        jnp.float32
    )
    channel_ids = lax.axis_index("tp") * channels + jnp.arange(channels, dtype=jnp.int32)
    group = channel_ids // (pool_width // 4)
    scaled = window_means(extended, position, group, tok_rows) * pool_scale
    squares = lax.psum(jnp.sum(scaled * scaled, axis=1), "tp")
    pooled_norm = (scaled * lax.rsqrt(squares / pool_width + epsilon)[:, None] * pool_gain).astype(
        jnp.bfloat16
    )
    moe_norm = row_norm(expert_input, moe_gain)
    shared_hidden = (
        jax.nn.silu(jnp.dot(moe_norm, shared_gate, preferred_element_type=jnp.float32))
        * jnp.dot(moe_norm, shared_up, preferred_element_type=jnp.float32)
    ).astype(jnp.bfloat16)
    pooled_all, shared_all = (
        lax.all_gather(pooled_norm, "tp", axis=1, tiled=True),
        lax.all_gather(shared_hidden, "tp", axis=1, tiled=True),
    )
    mix_out = jnp.dot(pooled_all, pool_out, preferred_element_type=jnp.float32).astype(jnp.bfloat16)
    shared_part = jnp.dot(shared_all, shared_down, preferred_element_type=jnp.float32)
    n_tok, top = route.shape
    local_experts = expert_gate.shape[0]
    experts = local_experts * lax.axis_size("ep")
    capacity = 2 * n_tok * top // experts
    flat_route = route.reshape(-1)
    table = (flat_route[:, None] == jnp.arange(experts, dtype=jnp.int32)[None, :]).astype(jnp.int32)
    ranks = jnp.sum((jnp.cumsum(table, axis=0) - table) * table, axis=1)
    slot = flat_route * capacity + ranks
    owner = (
        jnp.full((experts * capacity,), n_tok, jnp.int32)
        .at[slot]
        .set(jnp.arange(n_tok * top, dtype=jnp.int32) // top)
    )
    padded_rows = jnp.concatenate(
        [moe_norm, jnp.zeros((1, moe_norm.shape[1]), jnp.bfloat16)], axis=0
    )
    outgoing = padded_rows[owner].reshape(
        lax.axis_size("ep"), local_experts, capacity, moe_norm.shape[1]
    )
    middle = capacity // 2
    first = serve(outgoing[:, :, :middle], expert_gate, expert_up, expert_down)
    second = serve(outgoing[:, :, middle:], expert_gate, expert_up, expert_down)
    returned = jnp.concatenate([first, second], axis=2)
    back_rows = returned.reshape(experts * capacity, returned.shape[3])
    picked = back_rows[slot].reshape(n_tok, top, returned.shape[3]).astype(jnp.float32)
    weights = 2.5 * route_score / jnp.sum(route_score, axis=1, keepdims=True)
    routed = jnp.sum(picked * weights[:, :, None], axis=1)
    moe_out = (routed + shared_part).astype(jnp.bfloat16)
    return (mix_out, moe_out)


MESH = pl.DeviceIdType.MESH


def places():
    ep, tp = lax.axis_index("ep"), lax.axis_index("tp")
    z, core = ep // 2, ep % 2
    y, x = tp // 2, tp % 2
    return ep, tp, z, core, y * 2 + 1 - x, (1 - y) * 2 + x, (1 - y) * 2 + 1 - x


def aligned(start, size):
    return pl.ds(pl.multiple_of(start * size, size), size)


def fused_kernel(n_ep, n_tp, *refs):
    hbm, out_ref, rest = refs[:16], refs[16], refs[17:]
    (mi_h, ei_h, mg_h, eg_h, pi_h, ps_h, pg_h, po_h, rt_h, sc_h, wg_h, wu_h, wd_h, sg_h, su_h, sd_h) = hbm
    staged, rest = rest[:16], rest[16:]
    (mi, ei, mg, eg, pin, pscale, pgain, pout, rt, sc, wg, wu, wd, sg, su, sd) = staged
    (g, dense, mm, halo_s, halo_r, ext, sh_all, po_all, sq_all, hid) = rest[:10]
    (p, ca, s, bx, by, qx, qy, r, bz, o, so, lifted) = rest[10:22]
    pool = rest[22]
    ep, tp, z, core, xn, yn, dg = places()
    n_z = n_ep // 2
    last = n_z - 1
    counts = semaphore_counts(n_ep, n_tp)
    begins = {}
    for name in counts:
        begins[name] = sum(list(counts.values())[: list(counts).index(name)])

    def sem(name, index=0):
        return pool.at[begins[name] + index]

    rows, width = ei.shape
    cols = width // n_tp
    half = rows // 2
    f32, bf16 = jnp.float32, jnp.bfloat16
    other_core = z * 2 + 1 - core
    own_rows = aligned(ep, rows)
    low, high = pl.ds(0, half), pl.ds(half, half)

    loads = {}
    for number in (1, 3, 8, 9, 13, 14, 10, 11, 12, 0, 2, 4, 5, 6, 15, 7):
        loads[number] = pltpu.make_async_copy(hbm[number], staged[number], sem("load", number))
        loads[number].start()

    def send(src, dst, sem_s, sem_r, device):
        copy = pltpu.make_async_remote_copy(
            src_ref=src, dst_ref=dst, send_sem=sem_s, recv_sem=sem_r, device_id=device, device_id_type=MESH
        )
        copy.start()
        return copy

    halo = pltpu.make_async_remote_copy(
        src_ref=halo_s,
        dst_ref=halo_r,
        send_sem=sem("halo", 0),
        recv_sem=sem("halo", 1),
        device_id=((ep + 1) % n_ep, tp),
        device_id_type=MESH,
    )
    halo_r[...] = jnp.zeros_like(halo_r)
    lifted[...] = jnp.zeros_like(lifted)
    peers = (xn, yn, dg)
    upper_z, lower_z = jnp.minimum(z + 1, n_z - 1), jnp.maximum(z - 1, 0)
    upper, lower = (upper_z * 2 + core, tp), (lower_z * 2 + core, tp)
    has_upper, has_lower = z < n_z - 1, z > 0
    barrier = pltpu.get_barrier_semaphore()

    def knock(partner):
        pl.semaphore_signal(barrier, inc=1, device_id=partner, device_id_type=MESH)

    for partner in ((other_core, tp), (ep, xn), (ep, yn)):
        knock(partner)
    pl.when(has_upper)(lambda: knock(upper))
    pl.when(has_lower)(lambda: knock(lower))

    def norm_into(src, gain, dst, start, first_row, n_rows):
        step = 16

        def some(index, carry):
            row = pl.multiple_of(first_row + index * step, step)
            values = src[pl.ds(row, step), :].astype(f32)
            scale = lax.rsqrt(jnp.mean(values * values, axis=-1, keepdims=True) + epsilon)
            dst[pl.ds(pl.multiple_of(start + row, step), step), :] = (
                values * scale * gain[...]
            ).astype(bf16)
            return carry

        lax.fori_loop(0, n_rows // step, some, 0)

    side = jnp.where(core == 0, tp % 2, tp // 2)
    facing = jnp.where(core == 0, xn, yn)
    wide = width // 2

    def z_piece(plane, part, columns):
        start = pl.multiple_of((plane * 2 + core) * rows + part * half, half)
        return g.at[pl.ds(start, half), aligned(columns, wide)]

    def remote(piece, sem_s, sem_r, device):
        return pltpu.make_async_remote_copy(
            src_ref=piece, dst_ref=piece, send_sem=sem_s, recv_sem=sem_r, device_id=device, device_id_type=MESH
        )

    middle = has_upper & has_lower
    edge = jnp.logical_not(middle)

    def own_z(part):
        piece = z_piece(z, part, side)
        up = remote(piece, sem("own", 0), sem("z", z * 2 + part), upper)
        low_copy = remote(piece, sem("own", 1), sem("z", z * 2 + part), lower)
        return up, low_copy

    def start_own_z(part):
        up, low_copy = own_z(part)
        pl.when(middle)(up.start)
        pl.when(middle)(low_copy.start)
        inner = jnp.where(has_upper, upper_z, lower_z)
        straight = remote(
            z_piece(z, part, side), sem("own", 0), sem("z", z * 2 + part), (inner * 2 + core, tp)
        )
        pl.when(edge)(straight.start)

    def start_rest():
        inner = jnp.where(has_upper, upper_z, lower_z)
        for part in range(2):
            rest_copy = remote(
                z_piece(z, part, 1 - side),
                sem("own", 0),
                sem("e", (last - 1) * 2 + part),
                (inner * 2 + core, tp),
            )
            pl.when(edge)(rest_copy.start)

    def own_w():
        up = remote(dense.at[ep], sem("w_own", 0), sem("w", ep), upper)
        low_copy = remote(dense.at[ep], sem("w_own", 1), sem("w", ep), lower)
        return up, low_copy

    def start_own(pair):
        pl.when(has_upper)(pair[0].start)
        pl.when(has_lower)(pair[1].start)

    with jax.named_scope("norm"):
        loads[1].wait()
        loads[3].wait()
        norm_into(ei, eg, g, ep * rows, 0, half)
    with jax.named_scope("greet"):
        pl.semaphore_wait(barrier, 3 + jnp.where(has_upper, 1, 0) + jnp.where(has_lower, 1, 0))
    with jax.named_scope("norm2"):
        start_own_z(0)
        norm_into(ei, eg, g, ep * rows, half, half)
        start_own_z(1)
    whole = g.at[own_rows, :]
    gc = {0: send(whole, whole, sem("sent"), sem("own_pair"), (other_core, tp))}
    with jax.named_scope("dense"):
        loads[8].wait()
        loads[9].wait()
        total_score = jnp.sum(sc[...], axis=0, keepdims=True)
        expert_ids = lax.broadcasted_iota(jnp.int32, (n_ep, rows), 0)
        mine = jnp.zeros((n_ep, rows), f32)
        for choice in range(rt.shape[0]):
            share = 2.5 * sc[choice : choice + 1, :] / total_score
            mine = mine + jnp.where(rt[choice : choice + 1, :] == expert_ids, share, 0.0)
        dense[ep] = mine
        start_own(own_w())
        send(dense.at[ep], dense.at[ep], sem("w_over"), sem("w", ep), (other_core, tp))

    inner = jnp.where(2 * z < n_z, 1, -1)
    distance = [2 * jnp.maximum(z - q, q - z) - jnp.where((q - z) * inner > 0, 1, 0) for q in range(n_z)]
    planes = [0] * n_z
    for q in range(n_z):
        rank = 0
        for other in range(n_z):
            nearer = (distance[other] <= distance[q]) if other < q else (distance[other] < distance[q])
            rank = rank + jnp.where(nearer, 1, 0)
        for slot in range(n_z):
            planes[slot] = planes[slot] + jnp.where(rank == slot, q, 0)
    near, far = planes[n_z - 2], planes[n_z - 1]
    planes[n_z - 2] = jnp.where(middle, far, near)
    planes[n_z - 1] = jnp.where(middle, near, far)

    def z_forward(slot, part):
        plane = planes[slot]
        target = jnp.where(plane < z, z + 1, z - 1)
        valid = (target >= 0) & (target < n_z)
        safe = jnp.maximum(jnp.minimum(target, n_z - 1), 0)
        piece = z_piece(plane, part, side)
        return valid, remote(piece, sem("onward", slot - 1), sem("z", plane * 2 + part), (safe * 2 + core, tp))

    def w_forward(slot):
        plane = planes[slot]
        target = jnp.where(plane < z, z + 1, z - 1)
        safe = jnp.maximum(jnp.minimum(target, n_z - 1), 0)
        source = plane * 2 + core
        onward = remote(dense.at[source], sem("w_onward", slot - 1), sem("w", source), (safe * 2 + core, tp))
        over = remote(dense.at[source], sem("w_over"), sem("w", source), (other_core, tp))
        return onward, over

    def e_copy(slot, part):
        piece = z_piece(planes[slot], part, side)
        return remote(piece, sem("moved"), sem("e", (slot - 1) * 2 + part), (ep, facing))

    def d_copy(slot, part, late):
        piece = z_piece(planes[slot], part, 1 - side if late else side)
        return remote(piece, sem("moved"), sem("d", slot - 1), (other_core, tp))

    def z_arrive(slot, part, exchange=True):
        with jax.named_scope(f"z_arrive{slot}{part}"):
            valid, forward = z_forward(slot, part)
            forward.wait_recv()
            pl.when(valid)(forward.start)
            if exchange:
                e_copy(slot, part).start()
            d_copy(slot, part, 0).start()
            if part == 1:
                onward, over = w_forward(slot)
                onward.wait_recv()
                pl.when(valid)(onward.start)
                over.start()

    def full_arrive(slot, part):
        z_arrive(slot, part, False)

    def e_arrive(slot, part):
        with jax.named_scope(f"e_arrive{slot}{part}"):
            e_copy(slot, part).wait_recv()
            d_copy(slot, part, 1).start()

    def await_all(ref, name, index=0, received=False):
        copy = pltpu.make_async_remote_copy(
            src_ref=ref,
            dst_ref=ref,
            send_sem=sem(name, index),
            recv_sem=sem(name, index),
            device_id=(other_core, tp),
            device_id_type=MESH,
        )
        if received:
            copy.wait_recv()
        else:
            copy.wait_send()

    def block_of(n_rows, n_columns):
        return g.at[pl.ds(0, n_rows), pl.ds(0, n_columns)]

    def gather_drain():
        def own_sent(number):
            await_all(dense.at[0], "w_own", number)

        def onward_sent(slot):
            await_all(block_of(rows, wide), "onward", slot - 1)
            await_all(dense.at[0], "w_onward", slot - 1)

        pl.when(middle)(lambda: await_all(block_of(rows, wide), "own", 0))
        pl.when(middle)(lambda: await_all(block_of(rows, wide), "own", 1))
        pl.when(edge)(lambda: await_all(block_of(rows, width), "own", 0))
        pl.when(has_upper)(lambda: own_sent(0))
        pl.when(has_lower)(lambda: own_sent(1))
        for slot in range(1, n_z):
            valid, _ = z_forward(slot, 0)
            pl.when(valid)(lambda: onward_sent(slot))
        await_all(dense.at[pl.ds(0, n_z)], "w_over")

    with jax.named_scope("shared"):
        loads[13].wait()
        loads[14].wait()
        fs = sg.shape[1]
        tile = 256

        def shared_tile(index, carry):
            part = aligned(index, tile)
            gate = jnp.dot(g[own_rows, :], sg[:, part], preferred_element_type=f32)
            upper = jnp.dot(g[own_rows, :], su[:, part], preferred_element_type=f32)
            sh_all[:, pl.ds(pl.multiple_of(tp * fs + index * tile, tile), tile)] = (
                gate / (1.0 + jnp.exp(-gate)) * upper
            ).astype(bf16)
            return carry

        lax.fori_loop(0, fs // tile, shared_tile, 0)
    t_copies = {}

    def spread(kind, buffer):
        size = buffer.shape[1] // n_tp
        mine_slot = buffer.at[:, aligned(tp, size)]
        t_copies[kind, 0] = send(mine_slot, mine_slot, sem("sent"), sem("t", kind * 4), (ep, xn))
        t_copies[kind, 1] = send(mine_slot, mine_slot, sem("sent"), sem("t", kind * 4 + 1), (ep, yn))

    def spread_corner(kind, buffer):
        size = buffer.shape[1] // n_tp
        t_copies[kind, 0].wait_recv()
        part = buffer.at[low, aligned(xn, size)]
        t_copies[kind, 2] = send(part, part, sem("sent"), sem("t", kind * 4 + 2), (ep, yn))
        t_copies[kind, 1].wait_recv()
        part = buffer.at[high, aligned(yn, size)]
        t_copies[kind, 3] = send(part, part, sem("sent"), sem("t", kind * 4 + 3), (ep, xn))

    def corner_arrived(kind, buffer):
        size = buffer.shape[1] // n_tp
        for number in (2, 3):
            await_all(buffer.at[low, pl.ds(0, size)], "t", kind * 4 + number, True)

    spread(0, sh_all)

    channels = pin.shape[1]
    reach = halo_s.shape[0]
    def pool_project():
        with jax.named_scope("pool_in"):
            loads[0].wait()
            loads[2].wait()
            norm_into(mi, mg, mm, 0, 0, rows)
            loads[4].wait()
            pooled_in = jnp.dot(mm[...], pin[...], preferred_element_type=f32).astype(bf16)
            halo_s[...] = pooled_in[rows - reach :]
            ext[reach:, :] = pooled_in.astype(f32)
            pl.when(ep < n_ep - 1)(halo.start)

    eye = lax.broadcasted_iota(jnp.int32, (rows, rows), 0) == lax.broadcasted_iota(
        jnp.int32, (rows, rows), 1
    )

    def window():
        pl.when(ep > 0)(halo.wait_recv)
        ext[:reach, :] = halo_r[...].astype(f32)
        position = (ep * rows + 1 + lax.broadcasted_iota(jnp.int32, (rows, 1), 0)).astype(f32)
        total = jnp.zeros((rows, channels), f32)
        result = jnp.zeros((rows, channels), f32)
        for lag in range(reach):
            total = total + ext[reach - lag : reach - lag + rows, :]
            for index, size in enumerate(window_widths):
                if lag + 1 == size:
                    count = jnp.minimum(position, float(size))
                    result = jnp.where(tp == index, total / count, result)
        loads[5].wait()
        loads[6].wait()
        scaled = (result - ext[reach:, :]) * pscale[...]
        squares = jnp.sum(scaled * scaled, axis=1, keepdims=True)
        sq_all[tp] = jnp.sum(jnp.where(eye, squares, 0.0), axis=0, keepdims=True)
        po_all[:, aligned(tp, channels)] = (scaled * pgain[...]).astype(bf16)

    c_copies = {}
    fe = wg.shape[1]

    def hidden(k):
        plane = planes[k]
        with jax.named_scope(f"wait_over{k}"):
            if k == 0:
                gc[0].wait_recv()
            else:
                await_all(block_of(rows, width), "d", k - 1, True)
            source = plane * 2 + 1 - core
            remote(dense.at[source], sem("w_own", 0), sem("w", source), (other_core, tp)).wait_recv()
        with jax.named_scope(f"hidden{k}"):
            pair = aligned(plane, 2 * rows)
            factors = []
            for part in range(2):
                line = dense[plane * 2 + part, pl.ds(ep, 1), :]
                factors.append(jnp.sum(jnp.where(eye, line, 0.0), axis=1, keepdims=True))
            factor = jnp.concatenate(factors, axis=0)
            for index in range(fe // tile):
                part = pl.ds(index * tile, tile)
                gate = jnp.dot(g[pair, :], wg[:, part], preferred_element_type=f32)
                upper = jnp.dot(g[pair, :], wu[:, part], preferred_element_type=f32)
                hid[:, part] = (gate / (1.0 + jnp.exp(-gate)) * upper * factor).astype(bf16)

    quarters = (dg, yn, xn, tp)

    def down(k):
        with jax.named_scope(f"down{k}"):
            if k < last:
                for index in range(n_tp):
                    part = pl.ds(index * cols, cols)
                    p[k, :, part] = jnp.dot(hid[...], wd[:, part], preferred_element_type=f32).astype(bf16)
            if k < last:
                c_copies[k, 0] = send(
                    p.at[k, aligned(1 - core, rows), :], ca.at[k], sem("sent"), sem("c", k), (other_core, tp)
                )
            else:
                for number, quarter in enumerate(quarters):
                    part = aligned(quarter, cols)
                    p[k, :, part] = jnp.dot(hid[...], wd[:, part], preferred_element_type=f32).astype(bf16)
                    c_copies[k, number] = send(
                        p.at[k, aligned(1 - core, rows), part],
                        ca.at[k, :, part],
                        sem("sent"),
                        sem("c", k + number),
                        (other_core, tp),
                    )

    def cuts(k):
        return 1 if k == 1 else 2

    def place(k, cut):
        return sum(cuts(other) for other in range(k)) + cut

    def strip(k, quarter, cut):
        size = cols // cuts(k)
        return pl.ds(pl.multiple_of(quarter * cols + cut * size, size), size)

    def local_strip(k, cut):
        size = cols // cuts(k)
        return pl.ds(cut * size, size)

    def merge(k, number):
        if (k, number) in c_copies:
            c_copies[k, number].wait_recv()
        part = aligned(quarters[number], cols)
        own, theirs = p[k, aligned(core, rows), part].astype(f32), ca[k, :, part].astype(f32)
        if k == 0:
            own = own + lifted[:, part].astype(f32)
        s[k, :, part] = (own + theirs).astype(bf16)

    def first(k):
        with jax.named_scope(f"first{k}"):
            merge(k, 0)
            for cut in range(cuts(k)):
                here, there = strip(k, dg, cut), local_strip(k, cut)
                send(
                    s.at[k, low, here], bx.at[k, :, there], sem("moved"), sem("dx", place(k, cut)), (ep, xn)
                )
                send(
                    s.at[k, high, here], by.at[k, :, there], sem("moved"), sem("dy", place(k, cut)), (ep, yn)
                )
            for number in range(1, len(quarters)):
                merge(k, number)

    def lift():
        inner = jnp.where(has_upper, upper_z, lower_z)
        return pltpu.make_async_remote_copy(
            src_ref=s.at[1],
            dst_ref=lifted,
            send_sem=sem("lift", 0),
            recv_sem=sem("lift", 1),
            device_id=(inner * 2 + core, tp),
            device_id_type=MESH,
        )

    def lift_start():
        with jax.named_scope("lift"):
            for number in range(len(quarters)):
                merge(1, number)
            lift().start()

    def lift_arrive():
        with jax.named_scope("lift_wait"):
            lift().wait_recv()

    def second(k):
        with jax.named_scope(f"second{k}"):
            for cut in range(cuts(k)):
                there = local_strip(k, cut)
                here = strip(k, yn, cut)
                await_all(bx.at[k, :, there], "dx", place(k, cut), True)
                s[k, low, here] = (
                    s[k, low, here].astype(f32) + bx[k, :, there].astype(f32)
                ).astype(bf16)
                send(
                    s.at[k, :, here], qy.at[k, :, there], sem("moved"), sem("xy", place(k, cut)), (ep, yn)
                )
                here = strip(k, xn, cut)
                await_all(by.at[k, :, there], "dy", place(k, cut), True)
                s[k, high, here] = (
                    s[k, high, here].astype(f32) + by[k, :, there].astype(f32)
                ).astype(bf16)
                send(
                    s.at[k, :, here], qx.at[k, :, there], sem("moved"), sem("xy", place(k, cut)), (ep, xn)
                )

    def third(k):
        with jax.named_scope(f"third{k}"):
            for cut in range(cuts(k)):
                there = local_strip(k, cut)
                await_all(block_of(2 * rows, cols // cuts(k)), "xy", place(k, cut), True)
                total = (
                    s[k, :, strip(k, tp, cut)].astype(f32)
                    + qx[k, :, there].astype(f32)
                    + qy[k, :, there].astype(f32)
                )
                if k == 0:
                    o[:, there] = total
                else:
                    r[k, :, there] = total.astype(bf16)
                    send(
                        r.at[k, :, there],
                        bz.at[z, :, there],
                        sem("sent"),
                        sem("f", z),
                        (planes[k] * 2 + core, tp),
                    )


    def finish_t():
        with jax.named_scope("epilogue"):
            corner_arrived(1, po_all)
            await_all(sq_all.at[pl.ds(0, n_tp - 1)], "squares", 1, True)
            loads[15].wait()
            loads[7].wait()
            so[...] = jnp.dot(sh_all[...], sd[...], preferred_element_type=f32)
            mean = jnp.sum(sq_all[...], axis=0) / (channels * n_tp)
            inverse = lax.rsqrt(mean + epsilon)
            inverse = jnp.sum(jnp.where(eye, inverse, 0.0), axis=1, keepdims=True)
            out_ref[:rows] = (
                jnp.dot(po_all[...], pout[...], preferred_element_type=f32) * inverse
            ).astype(bf16)

    def spread_squares(number):
        line = sq_all.at[tp]
        send(line, line, sem("squares", 0), sem("squares", 1), (ep, peers[number]))

    def pooling():
        with jax.named_scope("window"):
            window()
        spread(1, po_all)
        for number in range(2):
            spread_squares(number)

    with jax.named_scope("weights_wait"):
        for number in (10, 11, 12):
            loads[number].wait()
    def on_edge(step, *which):
        pl.when(edge)(lambda: step(*which))

    def on_middle(step, *which):
        pl.when(middle)(lambda: step(*which))

    hidden(0)
    down(0)
    z_arrive(1, 0)
    start_rest()
    on_middle(full_arrive, 3, 0)
    pool_project()
    z_arrive(1, 1)
    on_middle(full_arrive, 3, 1)
    with jax.named_scope("spread_corner"):
        spread_corner(0, sh_all)
    e_arrive(1, 0)
    e_arrive(1, 1)
    pooling()
    z_arrive(2, 0)
    hidden(1)
    z_arrive(2, 1)
    down(1)
    on_edge(lift_start)
    on_middle(first, 1)
    with jax.named_scope("spread_corner"):
        spread_corner(1, po_all)
        for number in (2, 3):
            t_copies[0, number].wait_recv()
        spread_squares(2)
    e_arrive(2, 0)
    on_edge(z_arrive, 3, 0)
    on_edge(z_arrive, 3, 1)
    e_arrive(2, 1)
    hidden(2)
    on_middle(second, 1)
    down(2)
    finish_t()
    e_arrive(3, 0)
    e_arrive(3, 1)
    first(2)
    hidden(3)
    second(2)
    on_middle(third, 1)
    down(3)
    first(3)
    on_middle(lift_arrive)
    first(0)
    third(2)
    second(3)
    second(0)
    third(3)
    third(0)
    with jax.named_scope("final"):
        o[...] += so[...]

        def collect(k):
            source = planes[k]
            pltpu.make_async_remote_copy(
                src_ref=r.at[k],
                dst_ref=bz.at[source],
                send_sem=sem("sent"),
                recv_sem=sem("f", source),
                device_id=(source * 2 + core, tp),
                device_id_type=MESH,
            ).wait_recv()
            o[...] += bz[source].astype(f32)

        for k in range(1, last):
            collect(k)
        pl.when(edge)(lambda: collect(last))
        out_ref[rows:] = o[...].astype(bf16)
    with jax.named_scope("drain"):
        pl.when(ep < n_ep - 1)(halo.wait_send)
        gather_drain()
        await_all(sq_all.at[pl.ds(0, n_tp - 1)], "squares", 0)
        shared_rows = 3 * half * (sh_all.shape[1] + po_all.shape[1]) // (n_tp * width) * 2
        sent_rows = (n_z + 1) * rows + last * rows // n_tp + shared_rows
        moved_rows = 3 * half * last + 3 * half * n_z * 2 // n_tp

        def middle_sent():
            await_all(block_of(sent_rows, width), "sent")
            await_all(block_of(moved_rows - half, width), "moved")

        def edge_sent():
            await_all(block_of(sent_rows - rows // n_tp, width), "sent")
            await_all(block_of(moved_rows - 3 * half * 2 // n_tp, width), "moved")
            await_all(lifted, "lift", 0)

        pl.when(middle)(middle_sent)
        pl.when(edge)(edge_sent)


def semaphore_counts(n_ep, n_tp):
    n_z = n_ep // 2
    return {
        "load": 16, "own": 2, "w_own": 2, "onward": n_z - 1, "w_onward": n_z - 1, "w_over": 1,
        "sent": 1, "moved": 1, "z": 2 * n_z, "w": n_ep, "own_pair": 1, "e": 2 * (n_z - 1),
        "d": n_z - 1, "c": n_z - 1 + n_tp, "dx": 2 * n_z - 1, "dy": 2 * n_z - 1, "xy": 2 * n_z - 1, "f": n_z,
        "t": 8, "squares": 2, "halo": 2, "lift": 2,
    }


def dense_on_device(
    mix_input,
    expert_input,
    mix_gain,
    moe_gain,
    pool_in,
    pool_scale,
    pool_gain,
    pool_out,
    route,
    route_score,
    expert_gate,
    expert_up,
    expert_down,
    shared_gate,
    shared_up,
    shared_down,
):
    n_ep, n_tp = lax.axis_size("ep"), lax.axis_size("tp")
    n_z = n_ep // 2
    operands = (
        mix_input,
        expert_input,
        mix_gain.reshape(1, -1),
        moe_gain.reshape(1, -1),
        pool_in,
        pool_scale.reshape(1, -1),
        pool_gain.reshape(1, -1),
        pool_out,
        route.T,
        route_score.T,
        expert_gate[0],
        expert_up[0],
        expert_down[0],
        shared_gate,
        shared_up,
        shared_down,
    )
    rows, width = expert_input.shape
    cols = width // n_tp
    half = rows // 2
    channels = pool_in.shape[1]
    reach = reach_rows + 1
    f32, bf16 = jnp.float32, jnp.bfloat16
    scratch = [pltpu.VMEM(a.shape, a.dtype) for a in operands] + [
        pltpu.VMEM((n_ep * rows, width), bf16),
        pltpu.VMEM((n_ep, n_ep, rows), f32),
        pltpu.VMEM((rows, width), bf16),
        pltpu.VMEM((reach, channels), bf16),
        pltpu.VMEM((reach, channels), bf16),
        pltpu.VMEM((reach + rows, channels), f32),
        pltpu.VMEM((rows, n_tp * shared_gate.shape[1]), bf16),
        pltpu.VMEM((rows, n_tp * channels), bf16),
        pltpu.VMEM((n_tp, 1, rows), f32),
        pltpu.VMEM((2 * rows, expert_gate.shape[2]), bf16),
        pltpu.VMEM((n_z, 2 * rows, width), bf16),
        pltpu.VMEM((n_z, rows, width), bf16),
        pltpu.VMEM((n_z, rows, width), bf16),
        pltpu.VMEM((n_z, half, cols), bf16),
        pltpu.VMEM((n_z, half, cols), bf16),
        pltpu.VMEM((n_z, rows, cols), bf16),
        pltpu.VMEM((n_z, rows, cols), bf16),
        pltpu.VMEM((n_z, rows, cols), bf16),
        pltpu.VMEM((n_z, rows, cols), bf16),
        pltpu.VMEM((rows, cols), f32),
        pltpu.VMEM((rows, cols), f32),
        pltpu.VMEM((rows, width), bf16),
    ]
    sems = [pltpu.SemaphoreType.DMA((sum(semaphore_counts(n_ep, n_tp).values()),))]
    both = pl.pallas_call(
        lambda *refs: fused_kernel(n_ep, n_tp, *refs),
        out_shape=pltpu.VMEM((2 * rows, cols), bf16),
        in_specs=[pl.BlockSpec(memory_space=pltpu.HBM)] * len(operands),
        out_specs=pl.BlockSpec(memory_space=pltpu.VMEM),
        scratch_shapes=scratch + sems,
        compiler_params=pltpu.CompilerParams(
            collective_id=0, has_side_effects=True, vmem_limit_bytes=60 << 20
        ),
        name="fused",
    )(*operands)
    return both[:rows], both[rows:]
def chosen(*arrays):
    route, expert_gate = arrays[8], arrays[10]
    experts = expert_gate.shape[0] * lax.axis_size("ep")
    capacity = 2 * route.shape[0] * route.shape[1] // experts
    square = lax.axis_size("tp") == 4 and lax.axis_size("ep") == 2 * lax.axis_size("tp")
    if capacity == route.shape[0] and expert_gate.shape[0] == 1 and square:
        return dense_on_device(*arrays)
    return on_device(*arrays)


def solution(mesh):
    return jax.shard_map(
        chosen,
        mesh=mesh,
        in_specs=(
            P("ep", None),
            P("ep", None),
            P(),
            P(),
            P(None, "tp"),
            P("tp"),
            P("tp"),
            P(None, "tp"),
            P("ep", None),
            P("ep", None),
            P("ep", None, "tp"),
            P("ep", None, "tp"),
            P("ep", "tp", None),
            P(None, "tp"),
            P(None, "tp"),
            P(None, "tp"),
        ),
        out_specs=(P("ep", "tp"), P("ep", "tp")),
        check_vma=False,
    )
```
